256 devices in a mesh: ep: 128 (over z, y, x), tp: 2 (over core).
Axes of the slice: x: 4, y: 4, z: 8, core: 2. Of those that a mesh axis runs over, the one named last changes fastest.
Arguments:
- inputs: bfloat16 [2048, 1536], P('ep'), may hold values from -6 to 6
- norm_gain_attn: float32 [1536], replicated, may hold values from 0.1 to 1.9
- w_query: bfloat16 [1536, 768], P(None, 'tp'), may hold values from -0.15625 to 0.15625
- w_key: bfloat16 [1536, 128], P(None, 'tp'), may hold values from -0.15625 to 0.15625
- w_value: bfloat16 [1536, 128], P(None, 'tp'), may hold values from -0.15625 to 0.15625
- w_forget: bfloat16 [1536, 12], P(None, 'tp'), may hold values from -0.15625 to 0.15625
- forget_bias: float32 [12], P('tp'), may hold values from 0 to 3
- cache_keys: bfloat16 [2048, 2, 1024, 64], P('ep', 'tp'), may hold values from -250 to 250
- cache_values: bfloat16 [2048, 2, 1024, 64], P('ep', 'tp'), may hold values from -6 to 6
- cache_gates: float32 [2048, 12, 1024], P('ep', 'tp'), as said below
- lengths: int32 [2048], P('ep'), may hold values from 128 to 1024, as said below
- w_out: bfloat16 [768, 1536], P('tp'), may hold values from -0.21875 to 0.21875
- norm_gain_ffn: float32 [1536], replicated, may hold values from 0.1 to 1.9
- expert_ids: int32 [2048, 6], P('ep'), may hold values from 0 to 127, as said below
- group_weights: float32 [2048], P('ep'), may hold values from 0.2 to 1
- expert_weights: float32 [2048, 6], P('ep'), may hold values from 0.05 to 1
- exp_gate: bfloat16 [128, 1536, 512], P('ep', None, 'tp'), may hold values from -0.15625 to 0.15625
- exp_up: bfloat16 [128, 1536, 512], P('ep', None, 'tp'), may hold values from -0.15625 to 0.15625
- exp_down: bfloat16 [128, 512, 1536], P('ep', 'tp'), may hold values from -0.25 to 0.25
- dense_gate_vector: float32 [1536], replicated, may hold values from -0.15625 to 0.15625
- dense_gate_w: bfloat16 [1536, 16384], P(None, ('ep', 'tp')), may hold values from -0.15625 to 0.15625
- dense_up_w: bfloat16 [1536, 16384], P(None, ('ep', 'tp')), may hold values from -0.15625 to 0.15625
- dense_down_w: bfloat16 [16384, 1536], P(('ep', 'tp')), may hold values from -0.09375 to 0.09375
Outputs:
- mixed: bfloat16 [2048, 1536], P('ep', 'tp')
The draws below stay inside these ranges and needn't reach their ends.
Inputs may be any that keep to these rules, and one draw needn't show every extreme that they name: `cache_gates`: Non-increasing along positions. `lengths`: some sequence has 1024. `expert_ids`: each row names 6 different experts that share one group (the same quotient by 8). Among the rows of one index of ep at most 2 name the same expert, and some expert is named by exactly 2 rows of every index of ep.
All inputs are finite; a program needn't handle non-finite values.
Results may differ from the reference program's by a relative error of at most 0.013.
Values may be sent and summed in bfloat16 or wider, within the bound.
A program may use at most 128 MiB of HBM per device.

```python
import jax
import jax.numpy as jnp
from jax import lax

D = 1536
QUERY_HEAD_COUNT = 12
HEAD = 64
KV_HEADS = 2
EXP_FF = 512
EXP_PER_GROUP = 8
TOPK = 6
DENSE_FF = 16384
CACHE_LENGTH = 1024
SEQ_DEV = 16
SEQUENCE_COUNT = 2048
EXPERTS = 128
CAP = 2
N_EP = 128


def draw_cache_keys(key, part):
    base = jax.random.normal(jax.random.fold_in(key, 1), (SEQUENCE_COUNT, KV_HEADS, CACHE_LENGTH, HEAD), jnp.float32)
    return base.astype(jnp.bfloat16)


def draw_cache_gates(key, part):
    slow_share = 0.5
    lagging_head = jax.random.uniform(jax.random.fold_in(key, 11), (1, QUERY_HEAD_COUNT, 1), jnp.float32) < slow_share
    slow_rate = jax.random.uniform(jax.random.fold_in(key, 12), (SEQUENCE_COUNT, QUERY_HEAD_COUNT, 1), jnp.float32, 0.3, 1.5) / CACHE_LENGTH
    fast_rate = 1.0 / jax.random.uniform(jax.random.fold_in(key, 13), (SEQUENCE_COUNT, QUERY_HEAD_COUNT, 1), jnp.float32, 30.0, 100.0)
    rates = jnp.where(lagging_head, slow_rate, fast_rate)
    seq_factor = jnp.exp(jax.random.uniform(jax.random.fold_in(key, 14), (SEQUENCE_COUNT, 1, 1), jnp.float32, -0.7, 0.7))
    roughness = jax.random.uniform(jax.random.fold_in(key, 15), (SEQUENCE_COUNT, QUERY_HEAD_COUNT, CACHE_LENGTH), jnp.float32, 0.5, 1.5)
    length_steps = -rates * seq_factor * roughness
    spike_position = jax.random.randint(jax.random.fold_in(key, 16), (SEQUENCE_COUNT, 3), 0, CACHE_LENGTH)
    cache_positions = lax.broadcasted_iota(jnp.int32, (SEQUENCE_COUNT, CACHE_LENGTH), 1)
    spike_mask = jnp.any(cache_positions[:, :, None] == spike_position[:, None, :], axis=2)[:, None, :]
    spike_length = jax.random.uniform(jax.random.fold_in(key, 17), (SEQUENCE_COUNT, QUERY_HEAD_COUNT, CACHE_LENGTH), jnp.float32, 0.22, 0.69)
    length_steps = length_steps - jnp.where(spike_mask & lagging_head, spike_length, 0.0)
    return jnp.cumsum(length_steps, axis=2)


def draw_lengths(key, part):
    counts = jax.random.randint(jax.random.fold_in(key, 21), (SEQUENCE_COUNT,), CACHE_LENGTH // 8, CACHE_LENGTH + 1)
    chosen = jax.random.randint(jax.random.fold_in(key, 22), (), 0, SEQUENCE_COUNT)
    return jnp.where(jnp.arange(SEQUENCE_COUNT) == chosen, CACHE_LENGTH, counts).astype(jnp.int32)


def draw_expert_ids(key, part):
    n_groups = EXPERTS // EXP_PER_GROUP
    main_group = jax.random.randint(jax.random.fold_in(key, 31), (), 0, n_groups)
    main_expert = jax.random.randint(jax.random.fold_in(key, 32), (), 0, EXP_PER_GROUP)

    def one_block(block_key):
        ordering = jax.random.permutation(jax.random.fold_in(block_key, 1), n_groups)
        labels = (ordering - ordering[0] + main_group) % n_groups
        pool = jnp.repeat(labels, CAP)
        others = jax.random.permutation(jax.random.fold_in(block_key, 2), pool[CAP:])
        block_groups = jnp.concatenate([pool[:CAP], others])[:SEQ_DEV]
        token_order = jax.random.permutation(jax.random.fold_in(block_key, 3), SEQ_DEV)
        groups_here = block_groups[token_order]
        forced = token_order < CAP
        scores = jax.random.randint(jax.random.fold_in(block_key, 4), (SEQ_DEV, EXP_PER_GROUP), 0, 1 << 20) * EXP_PER_GROUP + jnp.arange(EXP_PER_GROUP)[None, :]
        ranking = jnp.argsort(scores, axis=1)
        picked = ranking[:, :TOPK]
        present = jnp.any(picked == main_expert, axis=1)
        replaced = picked.at[:, 0].set(main_expert)
        picked = jnp.where((forced & ~present)[:, None], replaced, picked)
        return groups_here[:, None] * EXP_PER_GROUP + picked
    block_keys = jax.random.split(jax.random.fold_in(key, 33), N_EP)
    return jax.vmap(one_block)(block_keys).reshape(SEQUENCE_COUNT, TOPK).astype(jnp.int32)


def level_of(key, dims, pieces, least, high):
    def one(position, shards_of):
        steps = jax.random.uniform(jax.random.fold_in(jax.random.fold_in(key, 6), position), (shards_of,), jnp.float32, least / len(pieces), high / len(pieces))
        return jnp.repeat(jnp.exp(steps), dims[position] // shards_of).reshape((-1,) + (1,) * (len(dims) - position - 1))

    level = one(*pieces[0])
    for cut in pieces[1:]:
        level = level * one(*cut)
    return level


def normal_values(own_key, extent, spread, bound, cuts=(), held_as=jnp.bfloat16):
    values = spread * jax.random.normal(own_key, extent, jnp.float32)
    if cuts:
        values = values * level_of(own_key, extent, cuts, -0.22, 0.18)
    return jnp.clip(values, -bound, bound).astype(held_as)


def setup_inputs(seed: int = 0) -> dict:
    seeds = jax.random.split(jax.random.key(seed), 24)
    return {
        "inputs": normal_values(seeds[0], (SEQUENCE_COUNT, D), 1.0, 6.0, ((0, 128),)),
        "norm_gain_attn": jnp.clip(1.0 + 0.18 * jax.random.normal(seeds[1], (D,), jnp.float32), 0.1, 1.9),
        "w_query": normal_values(seeds[2], (D, QUERY_HEAD_COUNT * HEAD), D ** -0.5, 0.15625, ((1, 2),)),
        "w_key": normal_values(seeds[3], (D, KV_HEADS * HEAD), D ** -0.5, 0.15625, ((1, 2),)),
        "w_value": normal_values(seeds[4], (D, KV_HEADS * HEAD), D ** -0.5, 0.15625, ((1, 2),)),
        "w_forget": normal_values(seeds[5], (D, QUERY_HEAD_COUNT), D ** -0.5, 0.15625, ((1, 2),)),
        "forget_bias": jnp.clip(3.0 * jax.random.uniform(seeds[6], (QUERY_HEAD_COUNT,), jnp.float32) ** level_of(seeds[6], (QUERY_HEAD_COUNT,), ((0, 2),), -0.2, 0.2), 0.0, 3.0),
        "cache_keys": draw_cache_keys(jax.random.fold_in(seeds[23], 71), 0),
        "cache_values": normal_values(seeds[8], (SEQUENCE_COUNT, KV_HEADS, CACHE_LENGTH, HEAD), 1.0, 6.0, ((0, 128), (1, 2))),
        "cache_gates": draw_cache_gates(jax.random.fold_in(seeds[23], 71), 0),
        "lengths": draw_lengths(jax.random.fold_in(seeds[23], 71), 0),
        "w_out": normal_values(seeds[11], (QUERY_HEAD_COUNT * HEAD, D), (QUERY_HEAD_COUNT * HEAD) ** -0.5, 0.21875, ((0, 2),)),
        "norm_gain_ffn": jnp.clip(1.0 + 0.18 * jax.random.normal(seeds[12], (D,), jnp.float32), 0.1, 1.9),
        "expert_ids": draw_expert_ids(jax.random.fold_in(seeds[23], 71), 0),
        "group_weights": jnp.clip(0.2 + 0.8 * jax.random.uniform(seeds[14], (SEQUENCE_COUNT,), jnp.float32) ** level_of(seeds[14], (SEQUENCE_COUNT,), ((0, 128),), -0.2, 0.2), 0.2, 1.0),
        "expert_weights": jnp.clip(0.05 + 0.95 * jax.random.uniform(seeds[15], (SEQUENCE_COUNT, TOPK), jnp.float32) ** level_of(seeds[15], (SEQUENCE_COUNT, TOPK), ((0, 128),), -0.2, 0.2), 0.05, 1.0),
        "exp_gate": normal_values(seeds[16], (EXPERTS, D, EXP_FF), D ** -0.5, 0.15625, ((0, 128), (2, 2))),
        "exp_up": normal_values(seeds[17], (EXPERTS, D, EXP_FF), D ** -0.5, 0.15625, ((0, 128), (2, 2))),
        "exp_down": normal_values(seeds[18], (EXPERTS, EXP_FF, D), EXP_FF ** -0.5, 0.25, ((0, 128), (1, 2))),
        "dense_gate_vector": normal_values(seeds[19], (D,), D ** -0.5, 0.15625, (), jnp.float32),
        "dense_gate_w": normal_values(seeds[20], (D, DENSE_FF), D ** -0.5, 0.15625, ((1, 256),)),
        "dense_up_w": normal_values(seeds[21], (D, DENSE_FF), D ** -0.5, 0.15625, ((1, 256),)),
        "dense_down_w": normal_values(seeds[22], (DENSE_FF, D), (DENSE_FF // 4) ** -0.5, 0.09375, ((0, 256),)),
    }


EPS = 1e-06

def rounded(values):
    return lax.optimization_barrier(values.astype(jnp.bfloat16)).astype(jnp.float32)

def rms_scale(row_block, gain):
    row_block = row_block.astype(jnp.float32)
    factor = lax.rsqrt(lax.optimization_barrier(jnp.mean(row_block * row_block, axis=-1, keepdims=True)) + EPS)
    return (row_block * factor * gain).astype(jnp.bfloat16)

def attend(bundle):
    queries, new_key, new_value, log_forget, keys, values, gates, counts = bundle
    seqs_here, kv_count, group_size, head_size = queries.shape
    cache_positions = lax.broadcasted_iota(jnp.int32, (1, 1, gates.shape[2]), 2)
    last_gate = lax.optimization_barrier(jnp.sum(jnp.where(cache_positions == (counts - 1)[:, None, None], gates, 0.0), axis=2))
    offsets = (last_gate + log_forget)[:, :, None] - gates
    offsets = offsets.reshape(seqs_here, kv_count, group_size, gates.shape[2])
    scale_factor = head_size ** (-0.5)
    query_wide = queries.astype(jnp.float32)
    cached = jnp.einsum('skgd,skld->skgl', query_wide, keys.astype(jnp.float32)) * scale_factor + offsets
    valid_mask = cache_positions.reshape(1, 1, 1, -1) < counts[:, None, None, None]
    cached = jnp.where(valid_mask, cached, -jnp.inf)
    own_score = lax.optimization_barrier(jnp.sum(query_wide * new_key.astype(jnp.float32)[:, :, None, :], axis=3)) * scale_factor
    peak_score = jnp.maximum(lax.optimization_barrier(jnp.max(cached, axis=3)), own_score)
    cached_exp = jnp.exp(cached - peak_score[..., None])
    own_exp = jnp.exp(own_score - peak_score)
    denominator = lax.optimization_barrier(jnp.sum(cached_exp, axis=3)) + own_exp
    cached_weight = (cached_exp / denominator[..., None]).astype(jnp.bfloat16)
    own_weight = (own_exp / denominator).astype(jnp.bfloat16)
    mixed_values = jnp.einsum('skgl,skld->skgd', cached_weight.astype(jnp.float32), values.astype(jnp.float32))
    mixed_values = mixed_values + own_weight.astype(jnp.float32)[..., None] * new_value.astype(jnp.float32)[:, :, None, :]
    return mixed_values.reshape(seqs_here, kv_count * group_size * head_size).astype(jnp.bfloat16)

def run_expert(bundle):
    row_block, gate_weight, up_weight, down_weight = bundle
    gate_part = jnp.dot(row_block, gate_weight, preferred_element_type=jnp.float32)
    up_part = jnp.dot(row_block, up_weight, preferred_element_type=jnp.float32)
    activated = (jax.nn.silu(gate_part) * up_part).astype(jnp.bfloat16)
    half_units = activated.shape[1] // 2
    first_part = rounded(jnp.dot(activated[:, :half_units], down_weight[:half_units], preferred_element_type=jnp.float32))
    second_part = rounded(jnp.dot(activated[:, half_units:], down_weight[half_units:], preferred_element_type=jnp.float32))
    return (first_part + second_part).astype(jnp.bfloat16)

def reference(inputs, norm_gain_attn, w_query, w_key, w_value, w_forget, forget_bias, cache_keys, cache_values, cache_gates, lengths, w_out, norm_gain_ffn, expert_ids, group_weights, expert_weights, exp_gate, exp_up, exp_down, dense_gate_vector, dense_gate_w, dense_up_w, dense_down_w):
    normed = rms_scale(inputs, norm_gain_attn)
    group_size = QUERY_HEAD_COUNT // KV_HEADS
    queries = jnp.dot(normed, w_query, preferred_element_type=jnp.float32).astype(jnp.bfloat16)
    new_keys = jnp.dot(normed, w_key, preferred_element_type=jnp.float32).astype(jnp.bfloat16)
    new_values = jnp.dot(normed, w_value, preferred_element_type=jnp.float32).astype(jnp.bfloat16)
    log_forget = jax.nn.log_sigmoid(jnp.dot(normed, w_forget, preferred_element_type=jnp.float32) + forget_bias)
    bundle = (queries.reshape(N_EP, SEQ_DEV, KV_HEADS, group_size, HEAD), new_keys.reshape(N_EP, SEQ_DEV, KV_HEADS, HEAD), new_values.reshape(N_EP, SEQ_DEV, KV_HEADS, HEAD), log_forget.reshape(N_EP, SEQ_DEV, QUERY_HEAD_COUNT), cache_keys.reshape(N_EP, SEQ_DEV, KV_HEADS, CACHE_LENGTH, HEAD), cache_values.reshape(N_EP, SEQ_DEV, KV_HEADS, CACHE_LENGTH, HEAD), cache_gates.reshape(N_EP, SEQ_DEV, QUERY_HEAD_COUNT, CACHE_LENGTH), lengths.reshape(N_EP, SEQ_DEV))
    heads_out = lax.map(attend, bundle).reshape(SEQUENCE_COUNT, QUERY_HEAD_COUNT * HEAD)
    half_heads = QUERY_HEAD_COUNT * HEAD // 2
    attn_out = rounded(jnp.dot(heads_out[:, :half_heads], w_out[:half_heads], preferred_element_type=jnp.float32))
    attn_out = attn_out + rounded(jnp.dot(heads_out[:, half_heads:], w_out[half_heads:], preferred_element_type=jnp.float32))
    after_attn = inputs.astype(jnp.float32) + attn_out
    normed_ffn = rms_scale(after_attn, norm_gain_ffn)
    flat_ids = expert_ids.reshape(-1).astype(jnp.int32)
    hit_table = (flat_ids[:, None] == jnp.arange(EXPERTS, dtype=jnp.int32)[None, :]).astype(jnp.int32)
    hit_blocks = hit_table.reshape(N_EP, SEQ_DEV * TOPK, EXPERTS)
    earlier = (jnp.cumsum(hit_blocks, axis=1) - hit_blocks).reshape(SEQUENCE_COUNT * TOPK, EXPERTS)
    slot_rank = lax.optimization_barrier(jnp.sum(earlier * hit_table, axis=1))
    source = jnp.arange(SEQUENCE_COUNT * TOPK, dtype=jnp.int32) // (SEQ_DEV * TOPK)
    slot_index = (source * CAP + slot_rank).astype(jnp.int32)
    repeated = jnp.repeat(normed_ffn, TOPK, axis=0)
    dispatched = jnp.zeros((EXPERTS, N_EP * CAP, D), jnp.bfloat16).at[flat_ids, slot_index].set(repeated)
    expert_rows = lax.map(run_expert, (dispatched, exp_gate, exp_up, exp_down))
    picked_rows = expert_rows[flat_ids, slot_index].astype(jnp.float32)
    route_weight = (group_weights[:, None] * expert_weights).reshape(SEQUENCE_COUNT * TOPK, 1)
    expert_mix = lax.optimization_barrier(jnp.sum((picked_rows * route_weight).reshape(SEQUENCE_COUNT, TOPK, D), axis=1))
    dense_gate = jnp.dot(normed_ffn, dense_gate_w, preferred_element_type=jnp.float32)
    dense_up = jnp.dot(normed_ffn, dense_up_w, preferred_element_type=jnp.float32)
    dense_hidden = (jax.nn.silu(dense_gate) * dense_up).astype(jnp.bfloat16)
    dense_out = jnp.dot(dense_hidden, dense_down_w, preferred_element_type=jnp.float32)
    gating = jax.nn.sigmoid(jnp.dot(normed_ffn.astype(jnp.float32), dense_gate_vector, precision=lax.Precision.HIGHEST))
    return (after_attn + expert_mix + gating[:, None] * dense_out).astype(jnp.bfloat16)
```

```python
import jax
import jax.numpy as jnp
from jax import lax
from jax.experimental import pallas as pl
from jax.experimental.pallas import tpu as pltpu
from jax.sharding import Mesh
from jax.sharding import PartitionSpec as P

EP = ("ep_0", "ep_1", "ep_2")
EP_TP = ("ep_0", "ep_1", "ep_2", "tp")


EPS = 1e-06


MESH = pl.DeviceIdType.MESH
WIDTH = 1536
HALF = WIDTH // 2
EXTRA = 128
ROW = WIDTH + EXTRA
ROWS = 16

K_PA = 0
K_ZG = 1
K_AU = 9
K_AV = 15
K_PUSH = 21
K_PART = 25
K_RV = 29
K_RU = 35
K_ZR = 41
N_SEM = 49


def mod4(value):
    return lax.rem(value + 8, 4)


def silu(value):
    return value / (1.0 + jnp.exp(-value))


def layer_kernel(
    pa_ref,
    inp_ref,
    gain_ref,
    route_ref,
    wg_ref,
    wu_ref,
    wd_ref,
    ed_ref,
    dd_ref,
    out_ref,
    pr,
    aa,
    xs,
    po,
    dr,
    va,
    vb,
    vf,
    sv,
    ua,
    ub,
    uf,
    su,
    zr,
    ssem,
    rsem,
):
    z = lax.axis_index("ep_0")
    y = lax.axis_index("ep_1")
    x = lax.axis_index("ep_2")
    t = lax.axis_index("tp")
    expert = (z * 4 + y) * 4 + x
    u = (1 - t) * y + t * x
    v = (1 - t) * x + t * y
    part = z // 4
    zz_own = lax.rem(z, 4)

    def near(du, dv):
        return (z, mod4(y + (1 - t) * du + t * dv), mod4(x + (1 - t) * dv + t * du), t)

    partner = (z, y, x, 1 - t)
    u_plus, u_minus = near(1, 0), near(-1, 0)
    v_plus, v_minus = near(0, 1), near(0, -1)

    def send(src, dst, k, device, kr=None):
        copy = pltpu.make_async_remote_copy(
            src_ref=src,
            dst_ref=dst,
            send_sem=ssem.at[k],
            recv_sem=rsem.at[k if kr is None else kr],
            device_id=device,
            device_id_type=MESH,
        )
        copy.start()
        return copy

    def landed(dst, k):
        pltpu.make_async_remote_copy(
            src_ref=dst,
            dst_ref=dst,
            send_sem=ssem.at[k],
            recv_sem=rsem.at[k],
            device_id=partner,
            device_id_type=MESH,
        ).wait_recv()

    barrier = pltpu.get_barrier_semaphore()
    for device in (partner, u_plus, u_minus, v_plus, v_minus):
        pl.semaphore_signal(barrier, inc=1, device_id=device, device_id_type=MESH)
    for dz in range(1, 8):
        for core in range(2):
            pl.semaphore_signal(
                barrier, inc=1, device_id=(lax.rem(z + dz, 8), y, x, core), device_id_type=MESH
            )
    pl.semaphore_wait(barrier, 19)

    sent = []

    sent.append(send(pa_ref, pr, K_PA, partner))
    landed(pr, K_PA)
    attn = pa_ref[...].astype(jnp.float32) + pr[...].astype(jnp.float32)
    after = inp_ref[...].astype(jnp.float32) + attn
    aa[...] = after
    factor = lax.rsqrt(jnp.mean(after * after, axis=-1, keepdims=True) + EPS)
    normed = (after * factor * gain_ref[...]).astype(jnp.bfloat16)

    @pl.when(part == t)
    def _():
        xs[0, v, zz_own, u, :, :WIDTH] = normed
        xs[0, v, zz_own, u, :, WIDTH:] = route_ref[...]
        block = xs.at[0, v, zz_own, u]
        for dz in (4, 3, 5, 2, 6, 1, 7):
            send(block, block, K_ZG + dz, (lax.rem(z + dz, 8), y, x, t), K_ZG + zz_own)

    for zz in range(4):

        @pl.when(4 * t + zz != z)
        def _():
            landed(xs.at[0, v, zz, u], K_ZG + zz)

    def ring_gather(piece, w, plus, minus, k):
        own_a, own_b = piece(0, w), piece(1, w)
        sent.append(send(own_a, own_a, k, plus))
        sent.append(send(own_b, own_b, k + 2, minus))
        sent.append(send(own_b, own_b, k + 1, plus))
        sent.append(send(own_a, own_a, k + 3, minus))

    def ring_relay(piece, w, plus, minus, k):
        a_left, b_right = piece(0, mod4(w - 1)), piece(1, mod4(w + 1))
        landed(a_left, k)
        sent.append(send(a_left, a_left, k + 4, plus))
        landed(b_right, k + 2)
        sent.append(send(b_right, b_right, k + 5, minus))

    def piece_u(half, w):
        return xs.at[0, v, pl.ds(2 * half, 2), w]

    def piece_v(half, w):
        return xs.at[0, w, pl.ds(2 * half, 2)]

    ring_gather(piece_u, u, u_plus, u_minus, K_AU)
    ring_relay(piece_u, u, u_plus, u_minus, K_AU)
    landed(piece_u(1, mod4(u - 1)), K_AU + 1)
    landed(piece_u(0, mod4(u + 1)), K_AU + 3)
    landed(piece_u(0, mod4(u + 2)), K_AU + 4)
    landed(piece_u(1, mod4(u + 2)), K_AU + 5)

    ring_gather(piece_v, v, v_plus, v_minus, K_AV)

    def push(w, slot):
        sent.append(send(xs.at[0, w], xs.at[1, w], K_PUSH + slot, partner))

    push(v, 0)

    lane = lax.broadcasted_iota(jnp.int32, (1, EXTRA), 1)

    def unit(side, w):
        rows = xs[side, w].reshape(16 * ROWS, ROW)
        tokens = rows[:, :WIDTH]
        weight = jnp.sum(
            jnp.where(lane == expert, rows[:, WIDTH:].astype(jnp.float32), 0.0),
            axis=1,
            keepdims=True,
        )
        gate = jnp.dot(tokens, wg_ref[...], preferred_element_type=jnp.float32)
        up = jnp.dot(tokens, wu_ref[...], preferred_element_type=jnp.float32)
        hidden = (silu(gate) * up * weight).astype(jnp.bfloat16)
        both = jnp.dot(tokens, wd_ref[...], preferred_element_type=jnp.float32)
        second = both[:, EXTRA:]
        logit = jnp.sum(
            jnp.where((lane >= 64) & (lane < 67), second, 0.0), axis=1, keepdims=True
        )
        gating = 1.0 / (1.0 + jnp.exp(-logit))
        dense = (silu(both[:, :EXTRA]) * second * gating).astype(jnp.bfloat16)
        total = jnp.dot(hidden, ed_ref[...], preferred_element_type=jnp.float32)
        total = total + jnp.dot(dense[:, :64], dd_ref[...], preferred_element_type=jnp.float32)
        po[side, w] = total.astype(jnp.bfloat16).reshape(4, 4, ROWS, WIDTH)

    def give(w, slot):
        sent.append(send(po.at[1, w], dr.at[w], K_PART + slot, partner))

    def received(w, slot):
        landed(xs.at[1, w], K_PUSH + slot)

    unit(0, v)
    received(u, 0)
    unit(1, u)
    give(u, 0)

    ring_relay(piece_v, v, v_plus, v_minus, K_AV)
    landed(piece_v(1, mod4(v - 1)), K_AV + 1)
    push(mod4(v - 1), 1)
    landed(piece_v(0, mod4(v + 1)), K_AV + 3)
    push(mod4(v + 1), 2)
    received(mod4(u - 1), 1)
    received(mod4(u + 1), 2)

    def middle(i, carry):
        side = i // 2
        w = mod4((1 - side) * v + side * u + 2 * lax.rem(i, 2) - 1)
        unit(side, w)
        return carry

    lax.fori_loop(0, 4, middle, 0)
    give(mod4(u - 1), 1)
    give(mod4(u + 1), 2)

    landed(piece_v(0, mod4(v + 2)), K_AV + 4)
    landed(piece_v(1, mod4(v + 2)), K_AV + 5)
    push(mod4(v + 2), 3)
    received(mod4(u + 2), 3)

    def last(i, carry):
        side = 1 - i
        unit(side, mod4((1 - side) * v + side * u + 2))
        return carry

    lax.fori_loop(0, 2, last, 0)
    give(mod4(u + 2), 3)

    f32 = jnp.float32
    bf16 = jnp.bfloat16

    def add_partner(w, slot):
        landed(dr.at[w], K_PART + slot)

        def body(i, carry):
            zz, uu = i // 4, lax.rem(i, 4)
            both = po[0, w, zz, uu].astype(f32) + dr[w, zz, uu].astype(f32)
            po[0, w, zz, uu] = both.astype(bf16)
            return carry

        lax.fori_loop(0, 16, body, 0)

    right, left, far = mod4(v + 1), mod4(v - 1), mod4(v + 2)
    low, high = pl.ds(0, 2), pl.ds(2, 2)
    add_partner(far, 3)
    sent.append(send(po.at[0, far, low], va, K_RV, v_plus))
    sent.append(send(po.at[0, far, high], vb, K_RV + 1, v_minus))
    add_partner(right, 2)
    sent.append(send(po.at[0, right, high], vf.at[1], K_RV + 2, v_plus))
    add_partner(left, 1)
    sent.append(send(po.at[0, left, low], vf.at[0], K_RV + 3, v_minus))
    add_partner(v, 0)

    landed(va, K_RV)

    def add_a(i, carry):
        zz, uu = i // 4, lax.rem(i, 4)
        po[0, right, zz, uu] = (
            po[0, right, zz, uu].astype(f32) + va[zz, uu].astype(f32)
        ).astype(bf16)
        return carry

    lax.fori_loop(0, 8, add_a, 0)
    sent.append(send(po.at[0, right, low], vf.at[2], K_RV + 4, v_plus))
    landed(vb, K_RV + 1)

    def add_b(i, carry):
        zz, uu = i // 4, lax.rem(i, 4)
        po[0, left, 2 + zz, uu] = (
            po[0, left, 2 + zz, uu].astype(f32) + vb[zz, uu].astype(f32)
        ).astype(bf16)
        return carry

    lax.fori_loop(0, 8, add_b, 0)
    sent.append(send(po.at[0, left, high], vf.at[3], K_RV + 5, v_minus))
    landed(vf.at[0], K_RV + 3)
    landed(vf.at[1], K_RV + 2)
    landed(vf.at[2], K_RV + 4)
    landed(vf.at[3], K_RV + 5)

    def add_v(i, carry):
        zz, uu = i // 4, lax.rem(i, 4)
        half, inner = zz // 2, lax.rem(zz, 2)
        total = (
            po[0, v, zz, uu].astype(f32)
            + vf[half, inner, uu].astype(f32)
            + vf[2 + half, inner, uu].astype(f32)
        )
        sv[uu, zz] = total.astype(bf16)
        return carry

    lax.fori_loop(0, 16, add_v, 0)

    right, left, far = mod4(u + 1), mod4(u - 1), mod4(u + 2)
    sent.append(send(sv.at[far, low], ua, K_RU, u_plus))
    sent.append(send(sv.at[far, high], ub, K_RU + 1, u_minus))
    sent.append(send(sv.at[right, high], uf.at[1], K_RU + 2, u_plus))
    sent.append(send(sv.at[left, low], uf.at[0], K_RU + 3, u_minus))
    landed(ua, K_RU)
    for zz in range(2):
        sv[right, zz] = (sv[right, zz].astype(f32) + ua[zz].astype(f32)).astype(bf16)
    sent.append(send(sv.at[right, low], uf.at[2], K_RU + 4, u_plus))
    landed(ub, K_RU + 1)
    for zz in range(2):
        sv[left, 2 + zz] = (sv[left, 2 + zz].astype(f32) + ub[zz].astype(f32)).astype(bf16)
    sent.append(send(sv.at[left, high], uf.at[3], K_RU + 5, u_minus))
    landed(uf.at[0], K_RU + 3)
    landed(uf.at[1], K_RU + 2)
    landed(uf.at[2], K_RU + 4)
    landed(uf.at[3], K_RU + 5)
    for zz in range(4):
        half, inner = zz // 2, zz % 2
        total = (
            sv[u, zz].astype(f32)
            + uf[half, inner].astype(f32)
            + uf[2 + half, inner].astype(f32)
        ).astype(bf16)
        for h in range(2):
            su[zz, h] = total[:, h * HALF : (h + 1) * HALF]

    for zz in range(4):
        for h in range(2):
            here = (4 * t + zz == z) & (t == h)

            @pl.when(jnp.logical_not(here))
            def _():
                send(
                    su.at[zz, h], zr.at[z], K_ZR + zz * 2 + h, (4 * t + zz, y, x, h), K_ZR + z
                )

            @pl.when(here)
            def _():
                zr[z] = su[zz, h]

    for s in range(8):

        @pl.when(jnp.logical_not((z == s) & (part == t)))
        def _():
            landed(zr.at[s], K_ZR + s)

    total = aa[:, pl.ds(pl.multiple_of(t * HALF, HALF), HALF)]
    for s in range(8):
        total = total + zr[s].astype(f32)
    out_ref[...] = total.astype(bf16)

    for copy in sent:
        copy.wait_send()

    def sent_out(src, k):
        pltpu.make_async_remote_copy(
            src_ref=src,
            dst_ref=src,
            send_sem=ssem.at[k],
            recv_sem=rsem.at[k],
            device_id=partner,
            device_id_type=MESH,
        ).wait_send()

    @pl.when(part == t)
    def _():
        for dz in range(1, 8):
            sent_out(xs.at[0, v, zz_own, u], K_ZG + dz)

    for zz in range(4):
        for h in range(2):

            @pl.when(jnp.logical_not((4 * t + zz == z) & (t == h)))
            def _():
                sent_out(su.at[zz, h], K_ZR + zz * 2 + h)


def run_layer(pa, inputs, gain, route, wg, wu, wd, ed, dd):
    bf16 = jnp.bfloat16
    vmem = pl.BlockSpec(memory_space=pltpu.VMEM)
    return pl.pallas_call(
        layer_kernel,
        out_shape=jax.ShapeDtypeStruct((ROWS, HALF), bf16),
        in_specs=[vmem] * 9,
        out_specs=vmem,
        scratch_shapes=[
            pltpu.VMEM((ROWS, WIDTH), bf16),
            pltpu.VMEM((ROWS, WIDTH), jnp.float32),
            pltpu.VMEM((2, 4, 4, 4, ROWS, ROW), bf16),
            pltpu.VMEM((2, 4, 4, 4, ROWS, WIDTH), bf16),
            pltpu.VMEM((4, 4, 4, ROWS, WIDTH), bf16),
            pltpu.VMEM((2, 4, ROWS, WIDTH), bf16),
            pltpu.VMEM((2, 4, ROWS, WIDTH), bf16),
            pltpu.VMEM((4, 2, 4, ROWS, WIDTH), bf16),
            pltpu.VMEM((4, 4, ROWS, WIDTH), bf16),
            pltpu.VMEM((2, ROWS, WIDTH), bf16),
            pltpu.VMEM((2, ROWS, WIDTH), bf16),
            pltpu.VMEM((4, 2, ROWS, WIDTH), bf16),
            pltpu.VMEM((4, 2, ROWS, HALF), bf16),
            pltpu.VMEM((8, ROWS, HALF), bf16),
            pltpu.SemaphoreType.DMA((N_SEM,)),
            pltpu.SemaphoreType.DMA((N_SEM,)),
        ],
        compiler_params=pltpu.CompilerParams(
            collective_id=0, has_side_effects=True, vmem_limit_bytes=52 * 1024 * 1024
        ),
        name="layer",
    )(pa, inputs, gain, route, wg, wu, wd, ed, dd)


def rms_scale(row_block, gain):
    row_block = row_block.astype(jnp.float32)
    factor = lax.rsqrt(jnp.mean(row_block * row_block, axis=-1, keepdims=True) + EPS)
    return (row_block * factor * gain).astype(jnp.bfloat16)


def attend(queries, new_key, new_value, log_forget, keys, values, gates, counts):
    seqs_here, kv_count, group_size, head_size = queries.shape
    cache_positions = lax.broadcasted_iota(jnp.int32, (1, 1, gates.shape[2]), 2)
    last_gate = jnp.sum(
        jnp.where(cache_positions == (counts - 1)[:, None, None], gates, 0.0), axis=2
    )
    offsets = (last_gate + log_forget)[:, :, None] - gates
    offsets = offsets.reshape(seqs_here, kv_count, group_size, gates.shape[2])
    scale_factor = head_size ** (-0.5)
    cached = (
        jnp.einsum("skgd,skld->skgl", queries, keys, preferred_element_type=jnp.float32)
        * scale_factor
        + offsets
    )
    valid_mask = cache_positions.reshape(1, 1, 1, -1) < counts[:, None, None, None]
    cached = jnp.where(valid_mask, cached, -jnp.inf)
    own_score = (
        jnp.einsum("skgd,skd->skg", queries, new_key, preferred_element_type=jnp.float32)
        * scale_factor
    )
    peak_score = jnp.maximum(jnp.max(cached, axis=3), own_score)
    cached_exp = jnp.exp(cached - peak_score[..., None])
    own_exp = jnp.exp(own_score - peak_score)
    denominator = jnp.sum(cached_exp, axis=3) + own_exp
    cached_weight = (cached_exp / denominator[..., None]).astype(jnp.bfloat16)
    own_weight = (own_exp / denominator).astype(jnp.bfloat16)
    mixed_values = jnp.einsum(
        "skgl,skld->skgd", cached_weight, values, preferred_element_type=jnp.float32
    )
    mixed_values = (
        mixed_values
        + own_weight.astype(jnp.float32)[..., None] * new_value.astype(jnp.float32)[:, :, None, :]
    )
    return mixed_values.reshape(seqs_here, kv_count * group_size * head_size).astype(jnp.bfloat16)


def shards(
    inputs,
    norm_gain_attn,
    w_query,
    w_key,
    w_value,
    w_forget,
    forget_bias,
    cache_keys,
    cache_values,
    cache_gates,
    lengths,
    w_out,
    norm_gain_ffn,
    expert_ids,
    group_weights,
    expert_weights,
    exp_gate,
    exp_up,
    exp_down,
    dense_gate_vector,
    dense_gate_w,
    dense_up_w,
    dense_down_w,
):
    seqs_here, model_width = inputs.shape
    kv_count = cache_keys.shape[1]
    head_size = cache_keys.shape[3]
    heads_here = w_forget.shape[1]
    group_size = heads_here // kv_count
    normed = rms_scale(inputs, norm_gain_attn)
    queries = jnp.dot(normed, w_query, preferred_element_type=jnp.float32).astype(jnp.bfloat16)
    queries = queries.reshape(seqs_here, kv_count, group_size, head_size)
    new_key = (
        jnp.dot(normed, w_key, preferred_element_type=jnp.float32)
        .astype(jnp.bfloat16)
        .reshape(seqs_here, kv_count, head_size)
    )
    new_value = (
        jnp.dot(normed, w_value, preferred_element_type=jnp.float32)
        .astype(jnp.bfloat16)
        .reshape(seqs_here, kv_count, head_size)
    )
    log_forget = jax.nn.log_sigmoid(
        jnp.dot(normed, w_forget, preferred_element_type=jnp.float32) + forget_bias
    )
    heads_out = attend(
        queries, new_key, new_value, log_forget, cache_keys, cache_values, cache_gates, lengths
    )
    partial_attn = jnp.dot(heads_out, w_out, preferred_element_type=jnp.float32)
    lanes = lax.broadcasted_iota(jnp.int32, (1, 1, EXTRA), 2)
    route_weight = group_weights[:, None] * expert_weights
    route = jnp.sum(
        jnp.where(expert_ids[:, :, None] == lanes, route_weight[:, :, None], 0.0), axis=1
    ).astype(jnp.bfloat16)
    first = lax.reduce_precision(dense_gate_vector, 8, 7)
    second = lax.reduce_precision(dense_gate_vector - first, 8, 7)
    third = dense_gate_vector - first - second
    vector = jnp.stack([first, second, third], axis=1).astype(jnp.bfloat16)
    wd = jnp.concatenate(
        [
            dense_gate_w,
            jnp.zeros((model_width, 64), jnp.bfloat16),
            dense_up_w,
            vector,
            jnp.zeros((model_width, 61), jnp.bfloat16),
        ],
        axis=1,
    )
    return run_layer(
        partial_attn.astype(jnp.bfloat16),
        inputs,
        norm_gain_ffn.reshape(1, -1),
        route,
        exp_gate[0],
        exp_up[0],
        wd,
        exp_down[0],
        dense_down_w,
    )


def solution(mesh):
    torus = Mesh(mesh.devices.reshape(8, 4, 4, mesh.shape["tp"]), ("ep_0", "ep_1", "ep_2", "tp"))
    placed = (
        P(EP, None),
        P(),
        P(None, "tp"),
        P(None, "tp"),
        P(None, "tp"),
        P(None, "tp"),
        P("tp"),
        P(EP, "tp", None, None),
        P(EP, "tp", None, None),
        P(EP, "tp", None),
        P(EP),
        P("tp", None),
        P(),
        P(EP, None),
        P(EP),
        P(EP, None),
        P(EP, None, "tp"),
        P(EP, None, "tp"),
        P(EP, "tp", None),
        P(),
        P(None, EP_TP),
        P(None, EP_TP),
        P(EP_TP, None),
    )
    return jax.shard_map(
        shards, mesh=torus, in_specs=placed, out_specs=P(EP, "tp"), check_vma=False
    )
```

```python
import jax
import jax.numpy as jnp
from jax import lax
from jax.experimental import pallas as pl
from jax.experimental.pallas import tpu as pltpu
from jax.sharding import Mesh
from jax.sharding import PartitionSpec as P

EP = ("ep_0", "ep_1", "ep_2")
EP_TP = ("ep_0", "ep_1", "ep_2", "tp")


EPS = 1e-06


MESH = pl.DeviceIdType.MESH
WIDTH = 1536
HALF = WIDTH // 2
EXTRA = 128
ROW = WIDTH + EXTRA
ROWS = 16

K_PA = 0
K_ZG = 1
K_AU = 9
K_AV = 15
K_PUSH = 21
K_PART = 28
K_RV = 35
K_RU = 45
K_ZR = 51
N_SEM = 59

PIECES = ((-1, 0), (1, 1), (-1, 1), (1, 0), (2, 0), (2, 1))


def mod4(value):
    return lax.rem(value + 8, 4)


def silu(value):
    return value / (1.0 + jnp.exp(-value))


def layer_kernel(
    pa_ref,
    inp_ref,
    gain_ref,
    route_ref,
    wg_ref,
    wu_ref,
    dg_ref,
    du_ref,
    vec_ref,
    ed_ref,
    dd_ref,
    out_ref,
    wd,
    down,
    pr,
    aa,
    xs,
    po,
    dr,
    va,
    vb,
    vf,
    sv,
    ua,
    ub,
    uf,
    su,
    zr,
    ssem,
    rsem,
):
    z = lax.axis_index("ep_0")
    y = lax.axis_index("ep_1")
    x = lax.axis_index("ep_2")
    t = lax.axis_index("tp")
    expert = (z * 4 + y) * 4 + x
    u = (1 - t) * y + t * x
    v = (1 - t) * x + t * y
    part = z // 4
    zz_own = lax.rem(z, 4)

    def near(du, dv):
        return (z, mod4(y + (1 - t) * du + t * dv), mod4(x + (1 - t) * dv + t * du), t)

    partner = (z, y, x, 1 - t)
    u_plus, u_minus = near(1, 0), near(-1, 0)
    v_plus, v_minus = near(0, 1), near(0, -1)

    def send(src, dst, k, device, kr=None):
        copy = pltpu.make_async_remote_copy(
            src_ref=src,
            dst_ref=dst,
            send_sem=ssem.at[k],
            recv_sem=rsem.at[k if kr is None else kr],
            device_id=device,
            device_id_type=MESH,
        )
        copy.start()
        return copy

    def landed(dst, k):
        pltpu.make_async_remote_copy(
            src_ref=dst,
            dst_ref=dst,
            send_sem=ssem.at[k],
            recv_sem=rsem.at[k],
            device_id=partner,
            device_id_type=MESH,
        ).wait_recv()

    barrier = pltpu.get_barrier_semaphore()
    for device in (partner, u_plus, u_minus, v_plus, v_minus):
        pl.semaphore_signal(barrier, inc=1, device_id=device, device_id_type=MESH)
    for dz in range(1, 8):
        for core in range(2):
            pl.semaphore_signal(
                barrier, inc=1, device_id=(lax.rem(z + dz, 8), y, x, core), device_id_type=MESH
            )
    pl.semaphore_wait(barrier, 19)

    sent = []

    sent.append(send(pa_ref, pr, K_PA, partner))
    landed(pr, K_PA)
    attn = pa_ref[...].astype(jnp.float32) + pr[...].astype(jnp.float32)
    after = inp_ref[...].astype(jnp.float32) + attn
    aa[...] = after
    factor = lax.rsqrt(jnp.mean(after * after, axis=-1, keepdims=True) + EPS)
    normed = (after * factor * gain_ref[...]).astype(jnp.bfloat16)

    @pl.when(part == t)
    def _():
        xs[0, v, zz_own, u, :, :WIDTH] = normed
        xs[0, v, zz_own, u, :, WIDTH:] = route_ref[...]
        block = xs.at[0, v, zz_own, u]
        for dz in (4, 3, 5, 2, 6, 1, 7):
            send(block, block, K_ZG + dz, (lax.rem(z + dz, 8), y, x, t), K_ZG + zz_own)

    vector = vec_ref[...]
    first = vector.astype(jnp.bfloat16).astype(jnp.float32)
    second = (vector - first).astype(jnp.bfloat16).astype(jnp.float32)
    third = vector - first - second
    line = lax.broadcasted_iota(jnp.int32, (ROWS, WIDTH), 0)
    stacked = jnp.where(line == 0, first, jnp.where(line == 1, second, third))
    wd[0:64] = dg_ref[...]
    wd[64:128] = jnp.zeros((64, WIDTH), jnp.bfloat16)
    wd[128:192] = du_ref[...]
    wd[192:208] = jnp.where(line < 3, stacked, 0.0).astype(jnp.bfloat16)
    wd[208:256] = jnp.zeros((48, WIDTH), jnp.bfloat16)
    down[0:256] = ed_ref[...]
    down[256:320] = dd_ref[...]
    down[320:384] = jnp.zeros((64, WIDTH), jnp.bfloat16)

    for zz in range(4):

        @pl.when(4 * t + zz != z)
        def _():
            landed(xs.at[0, v, zz, u], K_ZG + zz)

    def ring_gather(piece, w, plus, minus, k):
        own_a, own_b = piece(0, w), piece(1, w)
        sent.append(send(own_a, own_a, k, plus))
        sent.append(send(own_b, own_b, k + 2, minus))
        sent.append(send(own_b, own_b, k + 1, plus))
        sent.append(send(own_a, own_a, k + 3, minus))

    def ring_relay(piece, w, plus, minus, k):
        a_left, b_right = piece(0, mod4(w - 1)), piece(1, mod4(w + 1))
        landed(a_left, k)
        sent.append(send(a_left, a_left, k + 4, plus))
        landed(b_right, k + 2)
        sent.append(send(b_right, b_right, k + 5, minus))

    def piece_u(half, w):
        return xs.at[0, v, pl.ds(2 * half, 2), w]

    def piece_v(half, w):
        return xs.at[0, w, pl.ds(2 * half, 2)]

    ring_gather(piece_u, u, u_plus, u_minus, K_AU)
    ring_relay(piece_u, u, u_plus, u_minus, K_AU)
    landed(piece_u(1, mod4(u - 1)), K_AU + 1)
    landed(piece_u(0, mod4(u + 1)), K_AU + 3)
    landed(piece_u(0, mod4(u + 2)), K_AU + 4)
    landed(piece_u(1, mod4(u + 2)), K_AU + 5)

    ring_gather(piece_v, v, v_plus, v_minus, K_AV)

    f32 = jnp.float32
    bf16 = jnp.bfloat16
    lane = lax.broadcasted_iota(jnp.int32, (1, EXTRA), 1)

    def unit(side, one, two):
        (w_one, half_one), (w_two, half_two) = one, two
        rows = jnp.concatenate(
            [
                xs[side, w_one, 2 * half_one : 2 * half_one + 2].reshape(8 * ROWS, ROW),
                xs[side, w_two, 2 * half_two : 2 * half_two + 2].reshape(8 * ROWS, ROW),
            ],
            axis=0,
        )
        tokens = rows[:, :WIDTH]
        weight = jnp.sum(
            jnp.where(lane == expert, rows[:, WIDTH:].astype(f32), 0.0), axis=1, keepdims=True
        )
        gate = jnp.dot(tokens, wg_ref[...], preferred_element_type=f32)
        up = jnp.dot(tokens, wu_ref[...], preferred_element_type=f32)
        hidden = (silu(gate) * up * weight).astype(bf16)
        both = lax.dot_general(
            tokens, wd[...], (((1,), (1,)), ((), ())), preferred_element_type=f32
        )
        second_half = both[:, EXTRA:]
        logit = jnp.sum(
            jnp.where((lane >= 64) & (lane < 67), second_half, 0.0), axis=1, keepdims=True
        )
        gating = 1.0 / (1.0 + jnp.exp(-logit))
        dense = (silu(both[:, :EXTRA]) * second_half * gating).astype(bf16)
        hidden = jnp.concatenate([hidden, dense], axis=1)
        total = jnp.dot(hidden, down[...], preferred_element_type=f32).astype(bf16)
        total = total.reshape(2, 2, 4, ROWS, WIDTH)
        po[side, w_one, 2 * half_one : 2 * half_one + 2] = total[0]
        po[side, w_two, 2 * half_two : 2 * half_two + 2] = total[1]

    def half_of(half):
        return pl.ds(2 * half, 2)

    def piece_at(base, j):
        step, half = PIECES[j]
        return mod4(base + step), half

    def push(j):
        w, half = piece_at(v, j)
        piece = xs.at[0, w, half_of(half)]
        sent.append(send(piece, xs.at[1, w, half_of(half)], K_PUSH + 1 + j, partner))

    def received(j):
        w, half = piece_at(u, j)
        landed(xs.at[1, w, half_of(half)], K_PUSH + 1 + j)

    def give(j):
        w, half = piece_at(u, j)
        sent.append(
            send(po.at[1, w, half_of(half)], dr.at[w, half_of(half)], K_PART + 1 + j, partner)
        )

    def add_into(target, source, count):
        def body(i, carry):
            zz, uu = i // 4, lax.rem(i, 4)
            target[zz, uu] = (target[zz, uu].astype(f32) + source[zz, uu].astype(f32)).astype(bf16)
            return carry

        lax.fori_loop(0, 4 * count, body, 0)

    def take(j):
        w, half = piece_at(v, j)
        landed(dr.at[w, half_of(half)], K_PART + 1 + j)
        add_into(po.at[0, w, half_of(half)], dr.at[w, half_of(half)], 2)

    right, left, far = mod4(v + 1), mod4(v - 1), mod4(v + 2)

    sent.append(send(xs.at[0, v], xs.at[1, v], K_PUSH, partner))
    unit(0, (v, 0), (v, 1))
    landed(xs.at[1, u], K_PUSH)
    unit(1, (u, 0), (u, 1))
    sent.append(send(po.at[1, u], dr.at[u], K_PART, partner))

    ring_relay(piece_v, v, v_plus, v_minus, K_AV)
    push(0)
    push(1)
    unit(0, piece_at(v, 0), piece_at(v, 1))
    received(0)
    received(1)
    unit(1, piece_at(u, 0), piece_at(u, 1))
    give(0)
    give(1)

    landed(piece_v(1, left), K_AV + 1)
    push(2)
    landed(piece_v(0, right), K_AV + 3)
    push(3)
    unit(0, piece_at(v, 2), piece_at(v, 3))
    take(0)
    sent.append(send(po.at[0, left, half_of(0)], vf.at[0], K_RV + 1, v_minus))
    take(1)
    sent.append(send(po.at[0, right, half_of(1)], vf.at[1], K_RV, v_plus))
    received(2)
    received(3)
    unit(1, piece_at(u, 2), piece_at(u, 3))
    give(2)
    give(3)

    landed(piece_v(0, far), K_AV + 4)
    push(4)
    landed(piece_v(1, far), K_AV + 5)
    push(5)
    unit(0, piece_at(v, 4), piece_at(v, 5))
    received(4)
    received(5)
    unit(1, piece_at(u, 4), piece_at(u, 5))
    give(4)
    give(5)
    take(2)
    take(3)

    take(4)
    for i in range(2):
        sent.append(send(po.at[0, far, i], va.at[i], K_RV + 2 + i, v_plus))
    take(5)
    for i in range(2):
        sent.append(send(po.at[0, far, 2 + i], vb.at[i], K_RV + 4 + i, v_minus))
    landed(dr.at[v], K_PART)
    add_into(po.at[0, v], dr.at[v], 4)

    def add_row(target, source):
        def body(uu, carry):
            target[uu] = (target[uu].astype(f32) + source[uu].astype(f32)).astype(bf16)
            return carry

        lax.fori_loop(0, 4, body, 0)

    for i in range(2):
        landed(va.at[i], K_RV + 2 + i)
        add_row(po.at[0, right, i], va.at[i])
        sent.append(send(po.at[0, right, i], vf.at[2, i], K_RV + 6 + i, v_plus))
        landed(vb.at[i], K_RV + 4 + i)
        add_row(po.at[0, left, 2 + i], vb.at[i])
        sent.append(send(po.at[0, left, 2 + i], vf.at[3, i], K_RV + 8 + i, v_minus))
    landed(vf.at[0], K_RV + 1)
    landed(vf.at[1], K_RV)
    for i in range(2):
        landed(vf.at[2, i], K_RV + 6 + i)
        landed(vf.at[3, i], K_RV + 8 + i)

    def add_v(i, carry):
        zz, uu = i // 4, lax.rem(i, 4)
        half, inner = zz // 2, lax.rem(zz, 2)
        total = (
            po[0, v, zz, uu].astype(f32)
            + vf[half, inner, uu].astype(f32)
            + vf[2 + half, inner, uu].astype(f32)
        )
        sv[uu, zz] = total.astype(bf16)
        return carry

    lax.fori_loop(0, 16, add_v, 0)
    low, high = half_of(0), half_of(1)

    right, left, far = mod4(u + 1), mod4(u - 1), mod4(u + 2)
    sent.append(send(sv.at[far, low], ua, K_RU, u_plus))
    sent.append(send(sv.at[far, high], ub, K_RU + 1, u_minus))
    sent.append(send(sv.at[right, high], uf.at[1], K_RU + 2, u_plus))
    sent.append(send(sv.at[left, low], uf.at[0], K_RU + 3, u_minus))
    landed(ua, K_RU)
    for zz in range(2):
        sv[right, zz] = (sv[right, zz].astype(f32) + ua[zz].astype(f32)).astype(bf16)
    sent.append(send(sv.at[right, low], uf.at[2], K_RU + 4, u_plus))
    landed(ub, K_RU + 1)
    for zz in range(2):
        sv[left, 2 + zz] = (sv[left, 2 + zz].astype(f32) + ub[zz].astype(f32)).astype(bf16)
    sent.append(send(sv.at[left, high], uf.at[3], K_RU + 5, u_minus))
    landed(uf.at[0], K_RU + 3)
    landed(uf.at[1], K_RU + 2)
    landed(uf.at[2], K_RU + 4)
    landed(uf.at[3], K_RU + 5)
    for zz in range(4):
        half, inner = zz // 2, zz % 2
        total = (
            sv[u, zz].astype(f32)
            + uf[half, inner].astype(f32)
            + uf[2 + half, inner].astype(f32)
        ).astype(bf16)
        for h in range(2):
            su[zz, h] = total[:, h * HALF : (h + 1) * HALF]

    for zz in range(4):
        for h in range(2):
            here = (4 * t + zz == z) & (t == h)

            @pl.when(jnp.logical_not(here))
            def _():
                send(
                    su.at[zz, h], zr.at[z], K_ZR + zz * 2 + h, (4 * t + zz, y, x, h), K_ZR + z
                )

            @pl.when(here)
            def _():
                zr[z] = su[zz, h]

    for s in range(8):

        @pl.when(jnp.logical_not((z == s) & (part == t)))
        def _():
            landed(zr.at[s], K_ZR + s)

    total = aa[:, pl.ds(pl.multiple_of(t * HALF, HALF), HALF)]
    for s in range(8):
        total = total + zr[s].astype(f32)
    out_ref[...] = total.astype(bf16)

    for copy in sent:
        copy.wait_send()

    def sent_out(src, k):
        pltpu.make_async_remote_copy(
            src_ref=src,
            dst_ref=src,
            send_sem=ssem.at[k],
            recv_sem=rsem.at[k],
            device_id=partner,
            device_id_type=MESH,
        ).wait_send()

    @pl.when(part == t)
    def _():
        for dz in range(1, 8):
            sent_out(xs.at[0, v, zz_own, u], K_ZG + dz)

    for zz in range(4):
        for h in range(2):

            @pl.when(jnp.logical_not((4 * t + zz == z) & (t == h)))
            def _():
                sent_out(su.at[zz, h], K_ZR + zz * 2 + h)


def run_layer(pa, inputs, gain, route, wg, wu, dg, du, vector, ed, dd):
    bf16 = jnp.bfloat16
    vmem = pl.BlockSpec(memory_space=pltpu.VMEM)
    return pl.pallas_call(
        layer_kernel,
        out_shape=jax.ShapeDtypeStruct((ROWS, HALF), bf16),
        in_specs=[vmem] * 11,
        out_specs=vmem,
        scratch_shapes=[
            pltpu.VMEM((256, WIDTH), bf16),
            pltpu.VMEM((384, WIDTH), bf16),
            pltpu.VMEM((ROWS, WIDTH), bf16),
            pltpu.VMEM((ROWS, WIDTH), jnp.float32),
            pltpu.VMEM((2, 4, 4, 4, ROWS, ROW), bf16),
            pltpu.VMEM((2, 4, 4, 4, ROWS, WIDTH), bf16),
            pltpu.VMEM((4, 4, 4, ROWS, WIDTH), bf16),
            pltpu.VMEM((2, 4, ROWS, WIDTH), bf16),
            pltpu.VMEM((2, 4, ROWS, WIDTH), bf16),
            pltpu.VMEM((4, 2, 4, ROWS, WIDTH), bf16),
            pltpu.VMEM((4, 4, ROWS, WIDTH), bf16),
            pltpu.VMEM((2, ROWS, WIDTH), bf16),
            pltpu.VMEM((2, ROWS, WIDTH), bf16),
            pltpu.VMEM((4, 2, ROWS, WIDTH), bf16),
            pltpu.VMEM((4, 2, ROWS, HALF), bf16),
            pltpu.VMEM((8, ROWS, HALF), bf16),
            pltpu.SemaphoreType.DMA((N_SEM,)),
            pltpu.SemaphoreType.DMA((N_SEM,)),
        ],
        compiler_params=pltpu.CompilerParams(
            collective_id=0, has_side_effects=True, vmem_limit_bytes=52 * 1024 * 1024
        ),
        name="layer",
    )(pa, inputs, gain, route, wg, wu, dg, du, vector, ed, dd)


def rms_scale(row_block, gain):
    row_block = row_block.astype(jnp.float32)
    factor = lax.rsqrt(jnp.mean(row_block * row_block, axis=-1, keepdims=True) + EPS)
    return (row_block * factor * gain).astype(jnp.bfloat16)


def attend(queries, new_key, new_value, log_forget, keys, values, gates, counts):
    seqs_here, kv_count, group_size, head_size = queries.shape
    cache_positions = lax.broadcasted_iota(jnp.int32, (1, 1, gates.shape[2]), 2)
    last_gate = jnp.sum(
        jnp.where(cache_positions == (counts - 1)[:, None, None], gates, 0.0), axis=2
    )
    offsets = (last_gate + log_forget)[:, :, None] - gates
    offsets = offsets.reshape(seqs_here, kv_count, group_size, gates.shape[2])
    scale_factor = head_size ** (-0.5)
    cached = (
        jnp.einsum("skgd,skld->skgl", queries, keys, preferred_element_type=jnp.float32)
        * scale_factor
        + offsets
    )
    valid_mask = cache_positions.reshape(1, 1, 1, -1) < counts[:, None, None, None]
    cached = jnp.where(valid_mask, cached, -jnp.inf)
    own_score = (
        jnp.einsum("skgd,skd->skg", queries, new_key, preferred_element_type=jnp.float32)
        * scale_factor
    )
    peak_score = jnp.maximum(jnp.max(cached, axis=3), own_score)
    cached_exp = jnp.exp(cached - peak_score[..., None])
    own_exp = jnp.exp(own_score - peak_score)
    denominator = jnp.sum(cached_exp, axis=3) + own_exp
    cached_weight = (cached_exp / denominator[..., None]).astype(jnp.bfloat16)
    own_weight = (own_exp / denominator).astype(jnp.bfloat16)
    mixed_values = jnp.einsum(
        "skgl,skld->skgd", cached_weight, values, preferred_element_type=jnp.float32
    )
    mixed_values = (
        mixed_values
        + own_weight.astype(jnp.float32)[..., None] * new_value.astype(jnp.float32)[:, :, None, :]
    )
    return mixed_values.reshape(seqs_here, kv_count * group_size * head_size).astype(jnp.bfloat16)


def shards(
    inputs,
    norm_gain_attn,
    w_query,
    w_key,
    w_value,
    w_forget,
    forget_bias,
    cache_keys,
    cache_values,
    cache_gates,
    lengths,
    w_out,
    norm_gain_ffn,
    expert_ids,
    group_weights,
    expert_weights,
    exp_gate,
    exp_up,
    exp_down,
    dense_gate_vector,
    dense_gate_w,
    dense_up_w,
    dense_down_w,
):
    seqs_here, model_width = inputs.shape
    kv_count = cache_keys.shape[1]
    head_size = cache_keys.shape[3]
    heads_here = w_forget.shape[1]
    group_size = heads_here // kv_count
    normed = rms_scale(inputs, norm_gain_attn)
    queries = jnp.dot(normed, w_query, preferred_element_type=jnp.float32).astype(jnp.bfloat16)
    queries = queries.reshape(seqs_here, kv_count, group_size, head_size)
    new_key = (
        jnp.dot(normed, w_key, preferred_element_type=jnp.float32)
        .astype(jnp.bfloat16)
        .reshape(seqs_here, kv_count, head_size)
    )
    new_value = (
        jnp.dot(normed, w_value, preferred_element_type=jnp.float32)
        .astype(jnp.bfloat16)
        .reshape(seqs_here, kv_count, head_size)
    )
    log_forget = jax.nn.log_sigmoid(
        jnp.dot(normed, w_forget, preferred_element_type=jnp.float32) + forget_bias
    )
    heads_out = attend(
        queries, new_key, new_value, log_forget, cache_keys, cache_values, cache_gates, lengths
    )
    partial_attn = jnp.dot(heads_out, w_out, preferred_element_type=jnp.float32)
    lanes = lax.broadcasted_iota(jnp.int32, (1, 1, EXTRA), 2)
    route_weight = group_weights[:, None] * expert_weights
    route = jnp.sum(
        jnp.where(expert_ids[:, :, None] == lanes, route_weight[:, :, None], 0.0), axis=1
    ).astype(jnp.bfloat16)
    return run_layer(
        partial_attn.astype(jnp.bfloat16),
        inputs,
        norm_gain_ffn.reshape(1, -1),
        route,
        exp_gate[0],
        exp_up[0],
        dense_gate_w.T,
        dense_up_w.T,
        dense_gate_vector.reshape(1, -1),
        exp_down[0],
        dense_down_w,
    )


def solution(mesh):
    torus = Mesh(mesh.devices.reshape(8, 4, 4, mesh.shape["tp"]), ("ep_0", "ep_1", "ep_2", "tp"))
    placed = (
        P(EP, None),
        P(),
        P(None, "tp"),
        P(None, "tp"),
        P(None, "tp"),
        P(None, "tp"),
        P("tp"),
        P(EP, "tp", None, None),
        P(EP, "tp", None, None),
        P(EP, "tp", None),
        P(EP),
        P("tp", None),
        P(),
        P(EP, None),
        P(EP),
        P(EP, None),
        P(EP, None, "tp"),
        P(EP, None, "tp"),
        P(EP, "tp", None),
        P(),
        P(None, EP_TP),
        P(None, EP_TP),
        P(EP_TP, None),
    )
    return jax.shard_map(
        shards, mesh=torus, in_specs=placed, out_specs=P(EP, "tp"), check_vma=False
    )
```

```python
import jax
import jax.numpy as jnp
from jax import lax
from jax.experimental import pallas as pl
from jax.experimental.pallas import tpu as pltpu
from jax.sharding import Mesh
from jax.sharding import PartitionSpec as P

EP = ("ep_0", "ep_1", "ep_2")
EP_TP = ("ep_0", "ep_1", "ep_2", "tp")


EPS = 1e-06


MESH = pl.DeviceIdType.MESH
WIDTH = 1536
HALF = WIDTH // 2
EXTRA = 128
ROW = WIDTH + EXTRA
ROWS = 16

K_PA = 0
K_ZG = 1
K_AU = 9
K_ZR = 15
K_RU = 23
K_AV = 29
K_PUSH = 53
K_PART = 69
K_RV = 73
N_SEM = 97

STAGES = (0, 1, 2, -1)


def mod4(value):
    return lax.rem(value + 8, 4)


def silu(value):
    return value / (1.0 + jnp.exp(-value))


def layer_kernel(
    pa_ref,
    inp_ref,
    gain_ref,
    route_ref,
    wg_ref,
    wu_ref,
    dg_ref,
    du_ref,
    vec_ref,
    ed_ref,
    dd_ref,
    out_ref,
    wd,
    down,
    pr,
    aa,
    xs,
    po,
    dr,
    va,
    vb,
    vf,
    sv,
    ua,
    ub,
    uf,
    su,
    zr,
    ssem,
    rsem,
):
    z = lax.axis_index("ep_0")
    y = lax.axis_index("ep_1")
    x = lax.axis_index("ep_2")
    t = lax.axis_index("tp")
    expert = (z * 4 + y) * 4 + x
    u = (1 - t) * y + t * x
    v = (1 - t) * x + t * y
    part = z // 4
    zz_own = lax.rem(z, 4)

    def near(du, dv):
        return (z, mod4(y + (1 - t) * du + t * dv), mod4(x + (1 - t) * dv + t * du), t)

    partner = (z, y, x, 1 - t)
    u_plus, u_minus = near(1, 0), near(-1, 0)
    v_plus, v_minus = near(0, 1), near(0, -1)

    def send(src, dst, k, device, kr=None):
        copy = pltpu.make_async_remote_copy(
            src_ref=src,
            dst_ref=dst,
            send_sem=ssem.at[k],
            recv_sem=rsem.at[k if kr is None else kr],
            device_id=device,
            device_id_type=MESH,
        )
        copy.start()
        return copy

    def landed(dst, k):
        pltpu.make_async_remote_copy(
            src_ref=dst,
            dst_ref=dst,
            send_sem=ssem.at[k],
            recv_sem=rsem.at[k],
            device_id=partner,
            device_id_type=MESH,
        ).wait_recv()

    barrier = pltpu.get_barrier_semaphore()
    for device in (partner, u_plus, u_minus, v_plus, v_minus):
        pl.semaphore_signal(barrier, inc=1, device_id=device, device_id_type=MESH)
    for dz in range(1, 8):
        for core in range(2):
            pl.semaphore_signal(
                barrier, inc=1, device_id=(lax.rem(z + dz, 8), y, x, core), device_id_type=MESH
            )
    pl.semaphore_wait(barrier, 19)

    sent = []

    sent.append(send(pa_ref, pr, K_PA, partner))
    landed(pr, K_PA)
    attn = pa_ref[...].astype(jnp.float32) + pr[...].astype(jnp.float32)
    after = inp_ref[...].astype(jnp.float32) + attn
    aa[...] = after
    factor = lax.rsqrt(jnp.mean(after * after, axis=-1, keepdims=True) + EPS)
    normed = (after * factor * gain_ref[...]).astype(jnp.bfloat16)

    @pl.when(part == t)
    def _():
        xs[0, v, zz_own, u, :, :WIDTH] = normed
        xs[0, v, zz_own, u, :, WIDTH:] = route_ref[...]
        block = xs.at[0, v, zz_own, u]
        for dz in (4, 3, 5, 2, 6, 1, 7):
            send(block, block, K_ZG + dz, (lax.rem(z + dz, 8), y, x, t), K_ZG + zz_own)

    vector = vec_ref[...]
    first = vector.astype(jnp.bfloat16).astype(jnp.float32)
    second = (vector - first).astype(jnp.bfloat16).astype(jnp.float32)
    third = vector - first - second
    line = lax.broadcasted_iota(jnp.int32, (ROWS, WIDTH), 0)
    stacked = jnp.where(line == 0, first, jnp.where(line == 1, second, third))
    wd[0:64] = dg_ref[...]
    wd[64:128] = jnp.zeros((64, WIDTH), jnp.bfloat16)
    wd[128:192] = du_ref[...]
    wd[192:208] = jnp.where(line < 3, stacked, 0.0).astype(jnp.bfloat16)
    wd[208:256] = jnp.zeros((48, WIDTH), jnp.bfloat16)
    down[0:256] = ed_ref[...]
    down[256:320] = dd_ref[...]
    down[320:384] = jnp.zeros((64, WIDTH), jnp.bfloat16)

    for zz in range(4):

        @pl.when(4 * t + zz != z)
        def _():
            landed(xs.at[0, v, zz, u], K_ZG + zz)

    f32 = jnp.float32
    bf16 = jnp.bfloat16
    right, left, far = mod4(v + 1), mod4(v - 1), mod4(v + 2)
    low, high = pl.ds(0, 2), pl.ds(2, 2)

    def ring_send(piece, w, plus, minus, k):
        own_a, own_b = piece(low, w), piece(high, w)
        sent.append(send(own_a, own_a, k, plus))
        sent.append(send(own_b, own_b, k + 2, minus))
        sent.append(send(own_b, own_b, k + 1, plus))
        sent.append(send(own_a, own_a, k + 3, minus))

    def ring_relay(piece, w, plus, minus, k):
        a_left, b_right = piece(low, mod4(w - 1)), piece(high, mod4(w + 1))
        landed(a_left, k)
        sent.append(send(a_left, a_left, k + 4, plus))
        landed(b_right, k + 2)
        sent.append(send(b_right, b_right, k + 5, minus))

    def piece_u(half, w):
        return xs.at[0, v, half, w]

    def column(n):
        return mod4(u + STAGES[n])

    def piece_v(n):
        return lambda half, w: xs.at[0, w, half, column(n)]

    def push(n, w, slot):
        piece = xs.at[0, w, :, column(n)]
        sent.append(send(piece, xs.at[1, w, :, column(n)], K_PUSH + 4 * n + slot, partner))

    def gather_send(n):
        ring_send(piece_v(n), v, v_plus, v_minus, K_AV + 6 * n)
        push(n, v, 0)

    def gather_relay(n):
        ring_relay(piece_v(n), v, v_plus, v_minus, K_AV + 6 * n)

    def gather_near(n):
        landed(piece_v(n)(high, left), K_AV + 6 * n + 1)
        push(n, left, 1)
        landed(piece_v(n)(low, right), K_AV + 6 * n + 3)
        push(n, right, 2)

    def gather_far(n):
        landed(piece_v(n)(low, far), K_AV + 6 * n + 4)
        landed(piece_v(n)(high, far), K_AV + 6 * n + 5)
        push(n, far, 3)

    lane = lax.broadcasted_iota(jnp.int32, (1, EXTRA), 1)

    def unit(side, col):
        rows = xs[side, :, :, col].reshape(16 * ROWS, ROW)
        tokens = rows[:, :WIDTH]
        weight = jnp.sum(
            jnp.where(lane == expert, rows[:, WIDTH:].astype(f32), 0.0), axis=1, keepdims=True
        )
        gate = jnp.dot(tokens, wg_ref[...], preferred_element_type=f32)
        up = jnp.dot(tokens, wu_ref[...], preferred_element_type=f32)
        hidden = (silu(gate) * up * weight).astype(bf16)
        both = lax.dot_general(
            tokens, wd[...], (((1,), (1,)), ((), ())), preferred_element_type=f32
        )
        second_half = both[:, EXTRA:]
        logit = jnp.sum(
            jnp.where((lane >= 64) & (lane < 67), second_half, 0.0), axis=1, keepdims=True
        )
        gating = 1.0 / (1.0 + jnp.exp(-logit))
        dense = (silu(both[:, :EXTRA]) * second_half * gating).astype(bf16)
        hidden = jnp.concatenate([hidden, dense], axis=1)
        total = jnp.dot(hidden, down[...], preferred_element_type=f32).astype(bf16)
        po[side, :, :, col] = total.reshape(4, 4, ROWS, WIDTH)

    def own_unit(n):
        unit(0, column(n))

    def partner_unit(n):
        col = mod4(v + STAGES[n])
        for slot, step in enumerate((0, -1, 1, 2)):
            landed(xs.at[1, mod4(u + step), :, col], K_PUSH + 4 * n + slot)
        unit(1, col)
        sent.append(send(po.at[1, :, :, col], dr.at[:, :, col], K_PART + n, partner))

    def add_into(target, source, count):
        for i in range(count):
            target[i] = (target[i].astype(f32) + source[i].astype(f32)).astype(bf16)

    def reduce_send(n):
        col = column(n)
        k = K_RV + 6 * n
        landed(dr.at[:, :, col], K_PART + n)

        def take(w):
            add_into(po.at[0, w, :, col], dr.at[w, :, col], 4)

        take(far)
        sent.append(send(po.at[0, far, low, col], va.at[col], k, v_plus))
        sent.append(send(po.at[0, far, high, col], vb.at[col], k + 1, v_minus))
        take(right)
        sent.append(send(po.at[0, right, high, col], vf.at[1, col], k + 2, v_plus))
        take(left)
        sent.append(send(po.at[0, left, low, col], vf.at[0, col], k + 3, v_minus))

    def reduce_relay(n):
        col = column(n)
        k = K_RV + 6 * n
        landed(va.at[col], k)
        add_into(po.at[0, right, low, col], va.at[col], 2)
        sent.append(send(po.at[0, right, low, col], vf.at[2, col], k + 4, v_plus))
        landed(vb.at[col], k + 1)
        add_into(po.at[0, left, high, col], vb.at[col], 2)
        sent.append(send(po.at[0, left, high, col], vf.at[3, col], k + 5, v_minus))

    def reduce_end(n):
        col = column(n)
        k = K_RV + 6 * n
        landed(vf.at[0, col], k + 3)
        landed(vf.at[1, col], k + 2)
        landed(vf.at[2, col], k + 4)
        landed(vf.at[3, col], k + 5)
        for zz in range(4):
            half, inner = zz // 2, zz % 2
            total = (
                po[0, v, zz, col].astype(f32)
                + dr[v, zz, col].astype(f32)
                + vf[half, col, inner].astype(f32)
                + vf[2 + half, col, inner].astype(f32)
            )
            sv[col, zz] = total.astype(bf16)

    ring_send(piece_u, u, u_plus, u_minus, K_AU)
    gather_send(0)
    ring_relay(piece_u, u, u_plus, u_minus, K_AU)
    gather_relay(0)
    landed(piece_u(low, mod4(u + 1)), K_AU + 3)
    landed(piece_u(high, mod4(u - 1)), K_AU + 1)
    gather_send(1)
    landed(piece_u(low, mod4(u + 2)), K_AU + 4)
    landed(piece_u(high, mod4(u + 2)), K_AU + 5)
    gather_send(2)
    gather_near(0)
    gather_far(0)
    own_unit(0)
    gather_relay(1)
    gather_send(3)
    partner_unit(0)
    gather_near(1)
    gather_relay(2)
    reduce_send(0)
    gather_far(1)
    own_unit(1)
    gather_near(2)
    gather_relay(3)
    partner_unit(1)
    gather_far(2)
    own_unit(2)
    reduce_relay(0)
    reduce_send(1)
    gather_near(3)
    partner_unit(2)
    gather_far(3)
    own_unit(3)
    reduce_relay(1)
    reduce_send(2)
    partner_unit(3)
    reduce_end(0)
    reduce_end(1)

    up_col, far_col, down_col = column(1), column(2), column(3)
    sent.append(send(sv.at[up_col, high], uf.at[1], K_RU + 2, u_plus))
    reduce_relay(2)
    reduce_send(3)
    reduce_end(2)
    sent.append(send(sv.at[far_col, low], ua, K_RU, u_plus))
    sent.append(send(sv.at[far_col, high], ub, K_RU + 1, u_minus))
    reduce_relay(3)
    landed(ua, K_RU)
    add_into(sv.at[up_col, low], ua, 2)
    sent.append(send(sv.at[up_col, low], uf.at[2], K_RU + 4, u_plus))
    reduce_end(3)
    sent.append(send(sv.at[down_col, low], uf.at[0], K_RU + 3, u_minus))
    landed(ub, K_RU + 1)
    add_into(sv.at[down_col, high], ub, 2)
    sent.append(send(sv.at[down_col, high], uf.at[3], K_RU + 5, u_minus))
    landed(uf.at[1], K_RU + 2)
    landed(uf.at[2], K_RU + 4)
    landed(uf.at[3], K_RU + 5)
    landed(uf.at[0], K_RU + 3)
    for zz in range(4):
        half, inner = zz // 2, zz % 2
        total = (
            sv[u, zz].astype(f32)
            + uf[half, inner].astype(f32)
            + uf[2 + half, inner].astype(f32)
        ).astype(bf16)
        for h in range(2):
            su[zz, h] = total[:, h * HALF : (h + 1) * HALF]

    for zz in range(4):
        for h in range(2):
            here = (4 * t + zz == z) & (t == h)

            @pl.when(jnp.logical_not(here))
            def _():
                send(
                    su.at[zz, h], zr.at[z], K_ZR + zz * 2 + h, (4 * t + zz, y, x, h), K_ZR + z
                )

            @pl.when(here)
            def _():
                zr[z] = su[zz, h]

    for s in range(8):

        @pl.when(jnp.logical_not((z == s) & (part == t)))
        def _():
            landed(zr.at[s], K_ZR + s)

    total = aa[:, pl.ds(pl.multiple_of(t * HALF, HALF), HALF)]
    for s in range(8):
        total = total + zr[s].astype(f32)
    out_ref[...] = total.astype(bf16)

    for copy in sent:
        copy.wait_send()

    def sent_out(src, k):
        pltpu.make_async_remote_copy(
            src_ref=src,
            dst_ref=src,
            send_sem=ssem.at[k],
            recv_sem=rsem.at[k],
            device_id=partner,
            device_id_type=MESH,
        ).wait_send()

    @pl.when(part == t)
    def _():
        for dz in range(1, 8):
            sent_out(xs.at[0, v, zz_own, u], K_ZG + dz)

    for zz in range(4):
        for h in range(2):

            @pl.when(jnp.logical_not((4 * t + zz == z) & (t == h)))
            def _():
                sent_out(su.at[zz, h], K_ZR + zz * 2 + h)


def run_layer(pa, inputs, gain, route, wg, wu, dg, du, vector, ed, dd):
    bf16 = jnp.bfloat16
    vmem = pl.BlockSpec(memory_space=pltpu.VMEM)
    return pl.pallas_call(
        layer_kernel,
        out_shape=jax.ShapeDtypeStruct((ROWS, HALF), bf16),
        in_specs=[vmem] * 11,
        out_specs=vmem,
        scratch_shapes=[
            pltpu.VMEM((256, WIDTH), bf16),
            pltpu.VMEM((384, WIDTH), bf16),
            pltpu.VMEM((ROWS, WIDTH), bf16),
            pltpu.VMEM((ROWS, WIDTH), jnp.float32),
            pltpu.VMEM((2, 4, 4, 4, ROWS, ROW), bf16),
            pltpu.VMEM((2, 4, 4, 4, ROWS, WIDTH), bf16),
            pltpu.VMEM((4, 4, 4, ROWS, WIDTH), bf16),
            pltpu.VMEM((4, 2, ROWS, WIDTH), bf16),
            pltpu.VMEM((4, 2, ROWS, WIDTH), bf16),
            pltpu.VMEM((4, 4, 2, ROWS, WIDTH), bf16),
            pltpu.VMEM((4, 4, ROWS, WIDTH), bf16),
            pltpu.VMEM((2, ROWS, WIDTH), bf16),
            pltpu.VMEM((2, ROWS, WIDTH), bf16),
            pltpu.VMEM((4, 2, ROWS, WIDTH), bf16),
            pltpu.VMEM((4, 2, ROWS, HALF), bf16),
            pltpu.VMEM((8, ROWS, HALF), bf16),
            pltpu.SemaphoreType.DMA((N_SEM,)),
            pltpu.SemaphoreType.DMA((N_SEM,)),
        ],
        compiler_params=pltpu.CompilerParams(
            collective_id=0, has_side_effects=True, vmem_limit_bytes=52 * 1024 * 1024
        ),
        name="layer",
    )(pa, inputs, gain, route, wg, wu, dg, du, vector, ed, dd)


def rms_scale(row_block, gain):
    row_block = row_block.astype(jnp.float32)
    factor = lax.rsqrt(jnp.mean(row_block * row_block, axis=-1, keepdims=True) + EPS)
    return (row_block * factor * gain).astype(jnp.bfloat16)


def attend(queries, new_key, new_value, log_forget, keys, values, gates, counts):
    seqs_here, kv_count, group_size, head_size = queries.shape
    cache_positions = lax.broadcasted_iota(jnp.int32, (1, 1, gates.shape[2]), 2)
    last_gate = jnp.sum(
        jnp.where(cache_positions == (counts - 1)[:, None, None], gates, 0.0), axis=2
    )
    offsets = (last_gate + log_forget)[:, :, None] - gates
    offsets = offsets.reshape(seqs_here, kv_count, group_size, gates.shape[2])
    scale_factor = head_size ** (-0.5)
    cached = (
        jnp.einsum("skgd,skld->skgl", queries, keys, preferred_element_type=jnp.float32)
        * scale_factor
        + offsets
    )
    valid_mask = cache_positions.reshape(1, 1, 1, -1) < counts[:, None, None, None]
    cached = jnp.where(valid_mask, cached, -jnp.inf)
    own_score = (
        jnp.einsum("skgd,skd->skg", queries, new_key, preferred_element_type=jnp.float32)
        * scale_factor
    )
    peak_score = jnp.maximum(jnp.max(cached, axis=3), own_score)
    cached_exp = jnp.exp(cached - peak_score[..., None])
    own_exp = jnp.exp(own_score - peak_score)
    denominator = jnp.sum(cached_exp, axis=3) + own_exp
    cached_weight = (cached_exp / denominator[..., None]).astype(jnp.bfloat16)
    own_weight = (own_exp / denominator).astype(jnp.bfloat16)
    mixed_values = jnp.einsum(
        "skgl,skld->skgd", cached_weight, values, preferred_element_type=jnp.float32
    )
    mixed_values = (
        mixed_values
        + own_weight.astype(jnp.float32)[..., None] * new_value.astype(jnp.float32)[:, :, None, :]
    )
    return mixed_values.reshape(seqs_here, kv_count * group_size * head_size).astype(jnp.bfloat16)


def shards(
    inputs,
    norm_gain_attn,
    w_query,
    w_key,
    w_value,
    w_forget,
    forget_bias,
    cache_keys,
    cache_values,
    cache_gates,
    lengths,
    w_out,
    norm_gain_ffn,
    expert_ids,
    group_weights,
    expert_weights,
    exp_gate,
    exp_up,
    exp_down,
    dense_gate_vector,
    dense_gate_w,
    dense_up_w,
    dense_down_w,
):
    seqs_here, model_width = inputs.shape
    kv_count = cache_keys.shape[1]
    head_size = cache_keys.shape[3]
    heads_here = w_forget.shape[1]
    group_size = heads_here // kv_count
    normed = rms_scale(inputs, norm_gain_attn)
    queries = jnp.dot(normed, w_query, preferred_element_type=jnp.float32).astype(jnp.bfloat16)
    queries = queries.reshape(seqs_here, kv_count, group_size, head_size)
    new_key = (
        jnp.dot(normed, w_key, preferred_element_type=jnp.float32)
        .astype(jnp.bfloat16)
        .reshape(seqs_here, kv_count, head_size)
    )
    new_value = (
        jnp.dot(normed, w_value, preferred_element_type=jnp.float32)
        .astype(jnp.bfloat16)
        .reshape(seqs_here, kv_count, head_size)
    )
    log_forget = jax.nn.log_sigmoid(
        jnp.dot(normed, w_forget, preferred_element_type=jnp.float32) + forget_bias
    )
    heads_out = attend(
        queries, new_key, new_value, log_forget, cache_keys, cache_values, cache_gates, lengths
    )
    partial_attn = jnp.dot(heads_out, w_out, preferred_element_type=jnp.float32)
    lanes = lax.broadcasted_iota(jnp.int32, (1, 1, EXTRA), 2)
    route_weight = group_weights[:, None] * expert_weights
    route = jnp.sum(
        jnp.where(expert_ids[:, :, None] == lanes, route_weight[:, :, None], 0.0), axis=1
    ).astype(jnp.bfloat16)
    return run_layer(
        partial_attn.astype(jnp.bfloat16),
        inputs,
        norm_gain_ffn.reshape(1, -1),
        route,
        exp_gate[0],
        exp_up[0],
        dense_gate_w.T,
        dense_up_w.T,
        dense_gate_vector.reshape(1, -1),
        exp_down[0],
        dense_down_w,
    )


def solution(mesh):
    torus = Mesh(mesh.devices.reshape(8, 4, 4, mesh.shape["tp"]), ("ep_0", "ep_1", "ep_2", "tp"))
    placed = (
        P(EP, None),
        P(),
        P(None, "tp"),
        P(None, "tp"),
        P(None, "tp"),
        P(None, "tp"),
        P("tp"),
        P(EP, "tp", None, None),
        P(EP, "tp", None, None),
        P(EP, "tp", None),
        P(EP),
        P("tp", None),
        P(),
        P(EP, None),
        P(EP),
        P(EP, None),
        P(EP, None, "tp"),
        P(EP, None, "tp"),
        P(EP, "tp", None),
        P(),
        P(None, EP_TP),
        P(None, EP_TP),
        P(EP_TP, None),
    )
    return jax.shard_map(
        shards, mesh=torus, in_specs=placed, out_specs=P(EP, "tp"), check_vma=False
    )
```

```python
import jax
import jax.numpy as jnp
from jax import lax
from jax.experimental import pallas as pl
from jax.experimental.pallas import tpu as pltpu
from jax.sharding import Mesh
from jax.sharding import PartitionSpec as P

EP = ("ep_0", "ep_1", "ep_2")
EP_TP = ("ep_0", "ep_1", "ep_2", "tp")


EPS = 1e-06


MESH = pl.DeviceIdType.MESH
WIDTH = 1536
HALF = WIDTH // 2
EXTRA = 128
ROW = WIDTH + EXTRA
ROWS = 16

K_PA = 0
K_ZG = 1
K_AU = 9
K_ZR = 15
K_RU = 23
K_AV = 29
K_PUSH = 53
K_PART = 69
K_RV = 73
N_SEM = 97

STAGES = (0, 1, 2, -1)


def mod4(value):
    return lax.rem(value + 8, 4)


def silu(value):
    return value / (1.0 + jnp.exp(-value))


def att_scratch():
    bf16, f32 = jnp.bfloat16, jnp.float32
    return [
        pltpu.VMEM((1536, 384), bf16),
        pltpu.VMEM((16, 64, 1024), bf16),
        pltpu.VMEM((16, 64, 1024), bf16),
        pltpu.VMEM((6, 16, 1024), f32),
        pltpu.VMEM((384, 1536), bf16),
        pltpu.VMEM((128, 128), f32),
        pltpu.VMEM((1024, 128), f32),
        pltpu.SemaphoreType.DMA((8,)),
    ]


def att_copies(wq_hbm, ck_hbm, cv_hbm, cg_hbm, wo_hbm, wq, ck, cv, cg, wo, sem):
    half = pl.ds(0, 8), pl.ds(8, 8)
    pairs = [
        (wq_hbm, wq),
        (ck_hbm.at[half[0]], ck.at[half[0]]),
        (ck_hbm.at[half[1]], ck.at[half[1]]),
        (cg_hbm, cg),
        (cv_hbm.at[half[0]], cv.at[half[0]]),
        (cv_hbm.at[half[1]], cv.at[half[1]]),
        (wo_hbm, wo),
    ]
    return [pltpu.make_async_copy(src, dst, sem.at[i]) for i, (src, dst) in enumerate(pairs)]


def start_loads(wq_hbm, ck_hbm, cv_hbm, cg_hbm, wo_hbm, wq, ck, cv, cg, wo, qs, sc, sem):
    for copy in att_copies(wq_hbm, ck_hbm, cv_hbm, cg_hbm, wo_hbm, wq, ck, cv, cg, wo, sem):
        copy.start()


def attention(
    inp_ref,
    gain_ref,
    wk_ref,
    wv_ref,
    wf_ref,
    fb_ref,
    len_ref,
    wq_hbm,
    ck_hbm,
    cv_hbm,
    cg_hbm,
    wo_hbm,
    out_ref,
    wq,
    ck,
    cv,
    cg,
    wo,
    qs,
    sc,
    sem,
):
    f32, bf16 = jnp.float32, jnp.bfloat16
    loads = att_copies(wq_hbm, ck_hbm, cv_hbm, cg_hbm, wo_hbm, wq, ck, cv, cg, wo, sem)
    transposed = (((1,), (1,)), ((), ()))
    row_block = inp_ref[...].astype(f32)
    factor = lax.rsqrt(jnp.mean(row_block * row_block, axis=-1, keepdims=True) + EPS)
    normed = (row_block * factor * gain_ref[...].reshape(1, WIDTH)).astype(bf16)
    new_key = lax.dot_general(normed, wk_ref[...], transposed, preferred_element_type=f32)
    new_key = new_key.astype(bf16).astype(f32)
    new_value = lax.dot_general(normed, wv_ref[...], transposed, preferred_element_type=f32)
    new_value = new_value.astype(bf16).astype(f32)
    logit = lax.dot_general(normed, wf_ref[...], transposed, preferred_element_type=f32)
    loads[0].wait()
    queries = jnp.dot(normed, wq[...], preferred_element_type=f32).astype(bf16).astype(f32)
    own_scores = []
    qs[...] = jnp.zeros((128, 128), f32)

    def head_rows(h):
        return pl.ds(h, 16, stride=8)

    def load_head(h):
        return jnp.concatenate(
            [sc[pl.ds(128 * c + h, 16, stride=8), :] for c in range(8)], axis=1
        )

    for h in range(6):
        query = queries[:, 128 * (h // 2) : 128 * (h // 2) + 128]
        if h % 2:
            query = pltpu.roll(query, 64, 1)
        own_scores.append(jnp.sum(query[:, :64] * new_key, axis=1, keepdims=True) * 0.125)
        qs[head_rows(h), :] = query
    for s in range(16):
        if s % 8 == 0:
            loads[1 + s // 8].wait()
        scores = jnp.dot(
            qs[8 * s : 8 * s + 8, :64].astype(bf16), ck[s], preferred_element_type=f32
        )
        for c in range(8):
            sc[128 * c + 8 * s : 128 * c + 8 * s + 8, :] = scores[:, 128 * c : 128 * c + 128]
    loads[3].wait()
    line = lax.broadcasted_iota(jnp.int32, (16, 1), 0)
    counts = jnp.zeros((16, 1), jnp.int32)
    for s in range(16):
        counts = jnp.where(line == s, len_ref[s], counts)
    positions = lax.broadcasted_iota(jnp.int32, (16, 1024), 1)
    valid = positions < counts
    newest = positions == counts - 1
    own_weights = []
    for h in range(6):
        gates = cg[h]
        last = jnp.sum(jnp.where(newest, gates, 0.0), axis=1, keepdims=True)
        forget = logit[:, h : h + 1] + fb_ref[h]
        forget = jnp.minimum(forget, 0.0) - jnp.log1p(jnp.exp(-jnp.abs(forget)))
        offsets = (last + forget) - gates
        cached = load_head(h) * 0.125 + offsets
        cached = jnp.where(valid, cached, -jnp.inf)
        own = own_scores[h]
        peak = jnp.maximum(jnp.max(cached, axis=1, keepdims=True), own)
        cached = jnp.exp(cached - peak)
        own = jnp.exp(own - peak)
        denominator = jnp.sum(cached, axis=1, keepdims=True) + own
        cached = cached / denominator
        for c in range(8):
            sc[pl.ds(128 * c + h, 16, stride=8), :] = cached[:, 128 * c : 128 * c + 128]
        own_weights.append((own / denominator).astype(bf16).astype(f32))
    for s in range(16):
        if s % 8 == 0:
            loads[4 + s // 8].wait()
        weights = jnp.concatenate(
            [sc[128 * c + 8 * s : 128 * c + 8 * s + 8, :] for c in range(8)], axis=1
        )
        qs[8 * s : 8 * s + 8, :64] = lax.dot_general(
            weights.astype(bf16), cv[s], transposed, preferred_element_type=f32
        )
    loads[6].wait()
    total = jnp.zeros((16, 1536), f32)
    for h in range(6):
        head = qs[head_rows(h), :][:, :64] + own_weights[h] * new_value
        total = total + jnp.dot(
            head.astype(bf16), wo[64 * h : 64 * h + 64, :], preferred_element_type=f32
        )
    out_ref[...] = total.astype(bf16)


def layer_kernel(
    inp_ref,
    gain_attn_ref,
    wk_ref,
    wv_ref,
    wf_ref,
    fb_ref,
    len_ref,
    wq_hbm,
    ck_hbm,
    cv_hbm,
    cg_hbm,
    wo_hbm,
    gain_ref,
    ids_ref,
    gw_ref,
    ew_ref,
    wg_hbm,
    wu_hbm,
    ed_hbm,
    vec_ref,
    dg_hbm,
    du_hbm,
    dd_hbm,
    out_ref,
    wg_ref,
    wu_ref,
    pa_ref,
    route,
    wsem,
    wq,
    ck,
    cv,
    cg,
    wo,
    qs,
    sc,
    asem,
    wd,
    down,
    pr,
    aa,
    xs,
    po,
    dr,
    va,
    vb,
    vf,
    sv,
    ua,
    ub,
    uf,
    su,
    zr,
    ssem,
    rsem,
):
    z = lax.axis_index("ep_0")
    y = lax.axis_index("ep_1")
    x = lax.axis_index("ep_2")
    t = lax.axis_index("tp")
    expert = (z * 4 + y) * 4 + x
    u = (1 - t) * y + t * x
    v = (1 - t) * x + t * y
    part = z // 4
    zz_own = lax.rem(z, 4)

    def near(du, dv):
        return (z, mod4(y + (1 - t) * du + t * dv), mod4(x + (1 - t) * dv + t * du), t)

    partner = (z, y, x, 1 - t)
    u_plus, u_minus = near(1, 0), near(-1, 0)
    v_plus, v_minus = near(0, 1), near(0, -1)

    def send(src, dst, k, device, kr=None):
        copy = pltpu.make_async_remote_copy(
            src_ref=src,
            dst_ref=dst,
            send_sem=ssem.at[k],
            recv_sem=rsem.at[k if kr is None else kr],
            device_id=device,
            device_id_type=MESH,
        )
        copy.start()
        return copy

    def landed(dst, k):
        pltpu.make_async_remote_copy(
            src_ref=dst,
            dst_ref=dst,
            send_sem=ssem.at[k],
            recv_sem=rsem.at[k],
            device_id=partner,
            device_id_type=MESH,
        ).wait_recv()

    streams = (wq_hbm, ck_hbm, cv_hbm, cg_hbm, wo_hbm, wq, ck, cv, cg, wo)
    start_loads(*streams, qs, sc, asem)
    weight_loads = [
        pltpu.make_async_copy(src, dst, wsem.at[i])
        for i, (src, dst) in enumerate(
            (
                (wg_hbm, wg_ref),
                (wu_hbm, wu_ref),
                (ed_hbm, down.at[pl.ds(0, 256)]),
                (dd_hbm, down.at[pl.ds(256, 64)]),
                (dg_hbm, wd.at[pl.ds(0, 64)]),
                (du_hbm, wd.at[pl.ds(128, 64)]),
            )
        )
    ]
    for copy in weight_loads:
        copy.start()

    barrier = pltpu.get_barrier_semaphore()
    for device in (partner, u_plus, u_minus, v_plus, v_minus):
        pl.semaphore_signal(barrier, inc=1, device_id=device, device_id_type=MESH)
    for dz in range(1, 8):
        for core in range(2):
            pl.semaphore_signal(
                barrier, inc=1, device_id=(lax.rem(z + dz, 8), y, x, core), device_id_type=MESH
            )

    table_lane = lax.broadcasted_iota(jnp.int32, (1, EXTRA), 1)
    for s in range(ROWS):
        row = jnp.zeros((1, EXTRA), jnp.float32)
        for choice in range(6):
            row = jnp.where(
                table_lane == ids_ref[choice, s], gw_ref[s] * ew_ref[choice, s], row
            )
        route[s : s + 1, :] = row
    attention(
        inp_ref,
        gain_attn_ref,
        wk_ref,
        wv_ref,
        wf_ref,
        fb_ref,
        len_ref,
        wq_hbm,
        ck_hbm,
        cv_hbm,
        cg_hbm,
        wo_hbm,
        pa_ref,
        wq,
        ck,
        cv,
        cg,
        wo,
        qs,
        sc,
        asem,
    )
    pl.semaphore_wait(barrier, 19)

    sent = []

    sent.append(send(pa_ref, pr, K_PA, partner))
    landed(pr, K_PA)
    attn = pa_ref[...].astype(jnp.float32) + pr[...].astype(jnp.float32)
    after = inp_ref[...].astype(jnp.float32) + attn
    aa[...] = after
    factor = lax.rsqrt(jnp.mean(after * after, axis=-1, keepdims=True) + EPS)
    normed = (after * factor * gain_ref[...].reshape(1, WIDTH)).astype(jnp.bfloat16)

    @pl.when(part == t)
    def _():
        xs[0, v, zz_own, u, :, :WIDTH] = normed
        xs[0, v, zz_own, u, :, WIDTH:] = route[...].astype(jnp.bfloat16)
        block = xs.at[0, v, zz_own, u]
        for dz in (4, 3, 5, 2, 6, 1, 7):
            send(block, block, K_ZG + dz, (lax.rem(z + dz, 8), y, x, t), K_ZG + zz_own)

    vector = vec_ref[...].reshape(1, WIDTH)
    first = vector.astype(jnp.bfloat16).astype(jnp.float32)
    second = (vector - first).astype(jnp.bfloat16).astype(jnp.float32)
    third = vector - first - second
    line = lax.broadcasted_iota(jnp.int32, (ROWS, WIDTH), 0)
    stacked = jnp.where(line == 0, first, jnp.where(line == 1, second, third))
    wd[64:128] = jnp.zeros((64, WIDTH), jnp.bfloat16)
    wd[192:208] = jnp.where(line < 3, stacked, 0.0).astype(jnp.bfloat16)
    wd[208:256] = jnp.zeros((48, WIDTH), jnp.bfloat16)
    down[320:384] = jnp.zeros((64, WIDTH), jnp.bfloat16)
    for copy in weight_loads:
        copy.wait()

    for zz in range(4):

        @pl.when(4 * t + zz != z)
        def _():
            landed(xs.at[0, v, zz, u], K_ZG + zz)

    f32 = jnp.float32
    bf16 = jnp.bfloat16
    right, left, far = mod4(v + 1), mod4(v - 1), mod4(v + 2)
    low, high = pl.ds(0, 2), pl.ds(2, 2)

    def ring_send(piece, w, plus, minus, k):
        own_a, own_b = piece(low, w), piece(high, w)
        sent.append(send(own_a, own_a, k, plus))
        sent.append(send(own_b, own_b, k + 2, minus))
        sent.append(send(own_b, own_b, k + 1, plus))
        sent.append(send(own_a, own_a, k + 3, minus))

    def ring_relay(piece, w, plus, minus, k):
        a_left, b_right = piece(low, mod4(w - 1)), piece(high, mod4(w + 1))
        landed(a_left, k)
        sent.append(send(a_left, a_left, k + 4, plus))
        landed(b_right, k + 2)
        sent.append(send(b_right, b_right, k + 5, minus))

    def piece_u(half, w):
        return xs.at[0, v, half, w]

    def column(n):
        return mod4(u + STAGES[n])

    def piece_v(n):
        return lambda half, w: xs.at[0, w, half, column(n)]

    def push(n, w, slot):
        piece = xs.at[0, w, :, column(n)]
        sent.append(send(piece, xs.at[1, w, :, column(n)], K_PUSH + 4 * n + slot, partner))

    def gather_send(n):
        ring_send(piece_v(n), v, v_plus, v_minus, K_AV + 6 * n)
        push(n, v, 0)

    def gather_relay(n):
        ring_relay(piece_v(n), v, v_plus, v_minus, K_AV + 6 * n)

    def gather_near(n):
        landed(piece_v(n)(high, left), K_AV + 6 * n + 1)
        push(n, left, 1)
        landed(piece_v(n)(low, right), K_AV + 6 * n + 3)
        push(n, right, 2)

    def gather_far(n):
        landed(piece_v(n)(low, far), K_AV + 6 * n + 4)
        landed(piece_v(n)(high, far), K_AV + 6 * n + 5)
        push(n, far, 3)

    lane = lax.broadcasted_iota(jnp.int32, (1, EXTRA), 1)

    def unit(side, col):
        rows = xs[side, :, :, col].reshape(16 * ROWS, ROW)
        tokens = rows[:, :WIDTH]
        weight = jnp.sum(
            jnp.where(lane == expert, rows[:, WIDTH:].astype(f32), 0.0), axis=1, keepdims=True
        )
        gate = jnp.dot(tokens, wg_ref[...], preferred_element_type=f32)
        up = jnp.dot(tokens, wu_ref[...], preferred_element_type=f32)
        hidden = (silu(gate) * up * weight).astype(bf16)
        both = lax.dot_general(
            tokens, wd[...], (((1,), (1,)), ((), ())), preferred_element_type=f32
        )
        second_half = both[:, EXTRA:]
        logit = jnp.sum(
            jnp.where((lane >= 64) & (lane < 67), second_half, 0.0), axis=1, keepdims=True
        )
        gating = 1.0 / (1.0 + jnp.exp(-logit))
        dense = (silu(both[:, :EXTRA]) * second_half * gating).astype(bf16)
        hidden = jnp.concatenate([hidden, dense], axis=1)
        total = jnp.dot(hidden, down[...], preferred_element_type=f32).astype(bf16)
        po[side, :, :, col] = total.reshape(4, 4, ROWS, WIDTH)

    def own_unit(n):
        unit(0, column(n))

    def partner_unit(n):
        col = mod4(v + STAGES[n])
        for slot, step in enumerate((0, -1, 1, 2)):
            landed(xs.at[1, mod4(u + step), :, col], K_PUSH + 4 * n + slot)
        unit(1, col)
        sent.append(send(po.at[1, :, :, col], dr.at[:, :, col], K_PART + n, partner))

    def add_into(target, source, count):
        for i in range(count):
            target[i] = (target[i].astype(f32) + source[i].astype(f32)).astype(bf16)

    def reduce_send(n):
        col = column(n)
        k = K_RV + 6 * n
        landed(dr.at[:, :, col], K_PART + n)

        def take(w):
            add_into(po.at[0, w, :, col], dr.at[w, :, col], 4)

        take(far)
        sent.append(send(po.at[0, far, low, col], va.at[col], k, v_plus))
        sent.append(send(po.at[0, far, high, col], vb.at[col], k + 1, v_minus))
        take(right)
        sent.append(send(po.at[0, right, high, col], vf.at[1, col], k + 2, v_plus))
        take(left)
        sent.append(send(po.at[0, left, low, col], vf.at[0, col], k + 3, v_minus))

    def reduce_relay(n):
        col = column(n)
        k = K_RV + 6 * n
        landed(va.at[col], k)
        add_into(po.at[0, right, low, col], va.at[col], 2)
        sent.append(send(po.at[0, right, low, col], vf.at[2, col], k + 4, v_plus))
        landed(vb.at[col], k + 1)
        add_into(po.at[0, left, high, col], vb.at[col], 2)
        sent.append(send(po.at[0, left, high, col], vf.at[3, col], k + 5, v_minus))

    def reduce_end(n):
        col = column(n)
        k = K_RV + 6 * n
        landed(vf.at[0, col], k + 3)
        landed(vf.at[1, col], k + 2)
        landed(vf.at[2, col], k + 4)
        landed(vf.at[3, col], k + 5)
        for zz in range(4):
            half, inner = zz // 2, zz % 2
            total = (
                po[0, v, zz, col].astype(f32)
                + dr[v, zz, col].astype(f32)
                + vf[half, col, inner].astype(f32)
                + vf[2 + half, col, inner].astype(f32)
            )
            sv[col, zz] = total.astype(bf16)

    ring_send(piece_u, u, u_plus, u_minus, K_AU)
    gather_send(0)
    ring_relay(piece_u, u, u_plus, u_minus, K_AU)
    gather_relay(0)
    landed(piece_u(low, mod4(u + 1)), K_AU + 3)
    landed(piece_u(high, mod4(u - 1)), K_AU + 1)
    gather_send(1)
    landed(piece_u(low, mod4(u + 2)), K_AU + 4)
    landed(piece_u(high, mod4(u + 2)), K_AU + 5)
    gather_send(2)
    gather_near(0)
    gather_far(0)
    own_unit(0)
    gather_relay(1)
    gather_send(3)
    partner_unit(0)
    gather_near(1)
    gather_relay(2)
    reduce_send(0)
    gather_far(1)
    own_unit(1)
    gather_near(2)
    gather_relay(3)
    partner_unit(1)
    gather_far(2)
    own_unit(2)
    reduce_relay(0)
    reduce_send(1)
    gather_near(3)
    partner_unit(2)
    gather_far(3)
    own_unit(3)
    reduce_relay(1)
    reduce_send(2)
    partner_unit(3)
    reduce_end(0)
    reduce_end(1)

    up_col, far_col, down_col = column(1), column(2), column(3)
    sent.append(send(sv.at[up_col, high], uf.at[1], K_RU + 2, u_plus))
    reduce_relay(2)
    reduce_send(3)
    reduce_end(2)
    sent.append(send(sv.at[far_col, low], ua, K_RU, u_plus))
    sent.append(send(sv.at[far_col, high], ub, K_RU + 1, u_minus))
    reduce_relay(3)
    landed(ua, K_RU)
    add_into(sv.at[up_col, low], ua, 2)
    sent.append(send(sv.at[up_col, low], uf.at[2], K_RU + 4, u_plus))
    reduce_end(3)
    sent.append(send(sv.at[down_col, low], uf.at[0], K_RU + 3, u_minus))
    landed(ub, K_RU + 1)
    add_into(sv.at[down_col, high], ub, 2)
    sent.append(send(sv.at[down_col, high], uf.at[3], K_RU + 5, u_minus))
    landed(uf.at[1], K_RU + 2)
    landed(uf.at[2], K_RU + 4)
    landed(uf.at[3], K_RU + 5)
    landed(uf.at[0], K_RU + 3)
    for zz in range(4):
        half, inner = zz // 2, zz % 2
        total = (
            sv[u, zz].astype(f32)
            + uf[half, inner].astype(f32)
            + uf[2 + half, inner].astype(f32)
        ).astype(bf16)
        for h in range(2):
            su[zz, h] = total[:, h * HALF : (h + 1) * HALF]

    for zz in range(4):
        for h in range(2):
            here = (4 * t + zz == z) & (t == h)

            @pl.when(jnp.logical_not(here))
            def _():
                send(
                    su.at[zz, h], zr.at[z], K_ZR + zz * 2 + h, (4 * t + zz, y, x, h), K_ZR + z
                )

            @pl.when(here)
            def _():
                zr[z] = su[zz, h]

    for s in range(8):

        @pl.when(jnp.logical_not((z == s) & (part == t)))
        def _():
            landed(zr.at[s], K_ZR + s)

    total = aa[:, pl.ds(pl.multiple_of(t * HALF, HALF), HALF)]
    for s in range(8):
        total = total + zr[s].astype(f32)
    out_ref[...] = total.astype(bf16)

    for copy in sent:
        copy.wait_send()

    def sent_out(src, k):
        pltpu.make_async_remote_copy(
            src_ref=src,
            dst_ref=src,
            send_sem=ssem.at[k],
            recv_sem=rsem.at[k],
            device_id=partner,
            device_id_type=MESH,
        ).wait_send()

    @pl.when(part == t)
    def _():
        for dz in range(1, 8):
            sent_out(xs.at[0, v, zz_own, u], K_ZG + dz)

    for zz in range(4):
        for h in range(2):

            @pl.when(jnp.logical_not((4 * t + zz == z) & (t == h)))
            def _():
                sent_out(su.at[zz, h], K_ZR + zz * 2 + h)


def run_layer(*arrays):
    bf16 = jnp.bfloat16
    vmem = pl.BlockSpec(memory_space=pltpu.VMEM)
    smem = pl.BlockSpec(memory_space=pltpu.SMEM)
    hbm = pl.BlockSpec(memory_space=pl.ANY)
    return pl.pallas_call(
        layer_kernel,
        out_shape=jax.ShapeDtypeStruct((ROWS, HALF), bf16),
        in_specs=[vmem] * 5
        + [smem] * 2
        + [hbm] * 5
        + [vmem]
        + [smem] * 3
        + [hbm] * 3
        + [vmem]
        + [hbm] * 3,
        out_specs=vmem,
        scratch_shapes=[
            pltpu.VMEM((WIDTH, 256), bf16),
            pltpu.VMEM((WIDTH, 256), bf16),
            pltpu.VMEM((ROWS, WIDTH), bf16),
            pltpu.VMEM((ROWS, EXTRA), jnp.float32),
            pltpu.SemaphoreType.DMA((6,)),
            *att_scratch(),
            pltpu.VMEM((256, WIDTH), bf16),
            pltpu.VMEM((384, WIDTH), bf16),
            pltpu.VMEM((ROWS, WIDTH), bf16),
            pltpu.VMEM((ROWS, WIDTH), jnp.float32),
            pltpu.VMEM((2, 4, 4, 4, ROWS, ROW), bf16),
            pltpu.VMEM((2, 4, 4, 4, ROWS, WIDTH), bf16),
            pltpu.VMEM((4, 4, 4, ROWS, WIDTH), bf16),
            pltpu.VMEM((4, 2, ROWS, WIDTH), bf16),
            pltpu.VMEM((4, 2, ROWS, WIDTH), bf16),
            pltpu.VMEM((4, 4, 2, ROWS, WIDTH), bf16),
            pltpu.VMEM((4, 4, ROWS, WIDTH), bf16),
            pltpu.VMEM((2, ROWS, WIDTH), bf16),
            pltpu.VMEM((2, ROWS, WIDTH), bf16),
            pltpu.VMEM((4, 2, ROWS, WIDTH), bf16),
            pltpu.VMEM((4, 2, ROWS, HALF), bf16),
            pltpu.VMEM((8, ROWS, HALF), bf16),
            pltpu.SemaphoreType.DMA((N_SEM,)),
            pltpu.SemaphoreType.DMA((N_SEM,)),
        ],
        compiler_params=pltpu.CompilerParams(
            collective_id=0, has_side_effects=True, vmem_limit_bytes=60 * 1024 * 1024
        ),
        name="layer",
    )(*arrays)


def shards(
    inputs,
    norm_gain_attn,
    w_query,
    w_key,
    w_value,
    w_forget,
    forget_bias,
    cache_keys,
    cache_values,
    cache_gates,
    lengths,
    w_out,
    norm_gain_ffn,
    expert_ids,
    group_weights,
    expert_weights,
    exp_gate,
    exp_up,
    exp_down,
    dense_gate_vector,
    dense_gate_w,
    dense_up_w,
    dense_down_w,
):
    return run_layer(
        inputs,
        norm_gain_attn,
        w_key.T,
        w_value.T,
        w_forget.T,
        forget_bias,
        lengths,
        w_query,
        cache_keys[:, 0].transpose(0, 2, 1),
        cache_values[:, 0].transpose(0, 2, 1),
        cache_gates.transpose(1, 0, 2),
        w_out,
        norm_gain_ffn,
        expert_ids.T,
        group_weights,
        expert_weights.T,
        exp_gate[0],
        exp_up[0],
        exp_down[0],
        dense_gate_vector,
        dense_gate_w.T,
        dense_up_w.T,
        dense_down_w,
    )


def solution(mesh):
    torus = Mesh(mesh.devices.reshape(8, 4, 4, mesh.shape["tp"]), ("ep_0", "ep_1", "ep_2", "tp"))
    placed = (
        P(EP, None),
        P(),
        P(None, "tp"),
        P(None, "tp"),
        P(None, "tp"),
        P(None, "tp"),
        P("tp"),
        P(EP, "tp", None, None),
        P(EP, "tp", None, None),
        P(EP, "tp", None),
        P(EP),
        P("tp", None),
        P(),
        P(EP, None),
        P(EP),
        P(EP, None),
        P(EP, None, "tp"),
        P(EP, None, "tp"),
        P(EP, "tp", None),
        P(),
        P(None, EP_TP),
        P(None, EP_TP),
        P(EP_TP, None),
    )
    return jax.shard_map(
        shards, mesh=torus, in_specs=placed, out_specs=P(EP, "tp"), check_vma=False
    )
```

```python
import jax
import jax.numpy as jnp
from jax import lax
from jax.experimental import pallas as pl
from jax.experimental.pallas import tpu as pltpu
from jax.sharding import Mesh
from jax.sharding import PartitionSpec as P

EP = ("ep_0", "ep_1", "ep_2")
EP_TP = ("ep_0", "ep_1", "ep_2", "tp")


EPS = 1e-06


MESH = pl.DeviceIdType.MESH
WIDTH = 1536
HALF = WIDTH // 2
EXTRA = 128
ROW = WIDTH + EXTRA
ROWS = 16

K_PA = 0
K_ZG = 1
K_AU = 9
K_ZR = 15
K_RU = 23
K_AV = 29
K_PUSH = 53
K_PART = 69
K_RV = 73
N_SEM = 97

STAGES = (0, 1, 2, -1)


def mod4(value):
    return lax.rem(value + 8, 4)


def silu(value):
    return value / (1.0 + jnp.exp(-value))


def att_scratch():
    bf16, f32 = jnp.bfloat16, jnp.float32
    return [
        pltpu.VMEM((1536, 384), bf16),
        pltpu.VMEM((16, 64, 1024), bf16),
        pltpu.VMEM((16, 64, 1024), bf16),
        pltpu.VMEM((6, 16, 1024), f32),
        pltpu.VMEM((384, 1536), bf16),
        pltpu.VMEM((128, 128), f32),
        pltpu.VMEM((1024, 128), f32),
        pltpu.SemaphoreType.DMA((8,)),
    ]


def att_copies(wq_hbm, ck_hbm, cv_hbm, cg_hbm, wo_hbm, wq, ck, cv, cg, wo, sem):
    half = pl.ds(0, 8), pl.ds(8, 8)
    pairs = [
        (wq_hbm, wq),
        (ck_hbm.at[half[0]], ck.at[half[0]]),
        (ck_hbm.at[half[1]], ck.at[half[1]]),
        (cg_hbm, cg),
        (cv_hbm.at[half[0]], cv.at[half[0]]),
        (cv_hbm.at[half[1]], cv.at[half[1]]),
        (wo_hbm, wo),
    ]
    return [pltpu.make_async_copy(src, dst, sem.at[i]) for i, (src, dst) in enumerate(pairs)]


def start_loads(wq_hbm, ck_hbm, cv_hbm, cg_hbm, wo_hbm, wq, ck, cv, cg, wo, qs, sc, sem):
    for copy in att_copies(wq_hbm, ck_hbm, cv_hbm, cg_hbm, wo_hbm, wq, ck, cv, cg, wo, sem):
        copy.start()


def attention(
    inp_ref,
    gain_ref,
    wk_ref,
    wv_ref,
    wf_ref,
    fb_ref,
    len_ref,
    wq_hbm,
    ck_hbm,
    cv_hbm,
    cg_hbm,
    wo_hbm,
    out_ref,
    wq,
    ck,
    cv,
    cg,
    wo,
    qs,
    sc,
    sem,
):
    f32, bf16 = jnp.float32, jnp.bfloat16
    loads = att_copies(wq_hbm, ck_hbm, cv_hbm, cg_hbm, wo_hbm, wq, ck, cv, cg, wo, sem)
    transposed = (((1,), (1,)), ((), ()))
    row_block = inp_ref[...].astype(f32)
    factor = lax.rsqrt(jnp.mean(row_block * row_block, axis=-1, keepdims=True) + EPS)
    normed = (row_block * factor * gain_ref[...].reshape(1, WIDTH)).astype(bf16)
    new_key = lax.dot_general(normed, wk_ref[...], transposed, preferred_element_type=f32)
    new_key = new_key.astype(bf16).astype(f32)
    new_value = lax.dot_general(normed, wv_ref[...], transposed, preferred_element_type=f32)
    new_value = new_value.astype(bf16).astype(f32)
    logit = lax.dot_general(normed, wf_ref[...], transposed, preferred_element_type=f32)
    loads[0].wait()
    queries = jnp.dot(normed, wq[...], preferred_element_type=f32).astype(bf16).astype(f32)
    own_scores = []
    qs[...] = jnp.zeros((128, 128), f32)

    def head_rows(h):
        return pl.ds(h, 16, stride=8)

    def load_head(h):
        return jnp.concatenate(
            [sc[pl.ds(128 * c + h, 16, stride=8), :] for c in range(8)], axis=1
        )

    for h in range(6):
        query = queries[:, 128 * (h // 2) : 128 * (h // 2) + 128]
        if h % 2:
            query = pltpu.roll(query, 64, 1)
        own_scores.append(jnp.sum(query[:, :64] * new_key, axis=1, keepdims=True) * 0.125)
        qs[head_rows(h), :] = query
    for s in range(16):
        if s % 8 == 0:
            loads[1 + s // 8].wait()
        scores = jnp.dot(
            qs[8 * s : 8 * s + 8, :64].astype(bf16), ck[s], preferred_element_type=f32
        )
        for c in range(8):
            sc[128 * c + 8 * s : 128 * c + 8 * s + 8, :] = scores[:, 128 * c : 128 * c + 128]
    loads[3].wait()
    line = lax.broadcasted_iota(jnp.int32, (16, 1), 0)
    counts = jnp.zeros((16, 1), jnp.int32)
    for s in range(16):
        counts = jnp.where(line == s, len_ref[s], counts)
    positions = lax.broadcasted_iota(jnp.int32, (16, 1024), 1)
    valid = positions < counts
    newest = positions == counts - 1
    own_weights = []
    for h in range(6):
        gates = cg[h]
        last = jnp.sum(jnp.where(newest, gates, 0.0), axis=1, keepdims=True)
        forget = logit[:, h : h + 1] + fb_ref[h]
        forget = jnp.minimum(forget, 0.0) - jnp.log1p(jnp.exp(-jnp.abs(forget)))
        offsets = (last + forget) - gates
        cached = load_head(h) * 0.125 + offsets
        cached = jnp.where(valid, cached, -jnp.inf)
        own = own_scores[h]
        peak = jnp.maximum(jnp.max(cached, axis=1, keepdims=True), own)
        cached = jnp.exp(cached - peak)
        own = jnp.exp(own - peak)
        denominator = jnp.sum(cached, axis=1, keepdims=True) + own
        cached = cached / denominator
        for c in range(8):
            sc[pl.ds(128 * c + h, 16, stride=8), :] = cached[:, 128 * c : 128 * c + 128]
        own_weights.append((own / denominator).astype(bf16).astype(f32))
    for s in range(16):
        if s % 8 == 0:
            loads[4 + s // 8].wait()
        weights = jnp.concatenate(
            [sc[128 * c + 8 * s : 128 * c + 8 * s + 8, :] for c in range(8)], axis=1
        )
        qs[8 * s : 8 * s + 8, :64] = lax.dot_general(
            weights.astype(bf16), cv[s], transposed, preferred_element_type=f32
        )
    loads[6].wait()
    total = jnp.zeros((16, 1536), f32)
    for h in range(6):
        head = qs[head_rows(h), :][:, :64] + own_weights[h] * new_value
        total = total + jnp.dot(
            head.astype(bf16), wo[64 * h : 64 * h + 64, :], preferred_element_type=f32
        )
    out_ref[...] = total.astype(bf16)


def layer_kernel(
    inp_ref,
    gain_attn_ref,
    wk_ref,
    wv_ref,
    wf_ref,
    fb_ref,
    len_ref,
    wq_hbm,
    ck_hbm,
    cv_hbm,
    cg_hbm,
    wo_hbm,
    gain_ref,
    ids_ref,
    gw_ref,
    ew_ref,
    wg_hbm,
    wu_hbm,
    ed_hbm,
    vec_ref,
    dg_hbm,
    du_hbm,
    dd_hbm,
    out_ref,
    wg_ref,
    wu_ref,
    pa_ref,
    route,
    wsem,
    wq,
    ck,
    cv,
    cg,
    wo,
    qs,
    sc,
    asem,
    wd,
    down,
    pr,
    aa,
    xs,
    po,
    dr,
    va,
    vb,
    vf,
    sv,
    ua,
    ub,
    uf,
    su,
    zr,
    ssem,
    rsem,
):
    z = lax.axis_index("ep_0")
    y = lax.axis_index("ep_1")
    x = lax.axis_index("ep_2")
    t = lax.axis_index("tp")
    expert = (z * 4 + y) * 4 + x
    u = (1 - t) * y + t * x
    v = (1 - t) * x + t * y
    part = z // 4
    zz_own = lax.rem(z, 4)

    def near(du, dv):
        return (z, mod4(y + (1 - t) * du + t * dv), mod4(x + (1 - t) * dv + t * du), t)

    partner = (z, y, x, 1 - t)
    u_plus, u_minus = near(1, 0), near(-1, 0)
    v_plus, v_minus = near(0, 1), near(0, -1)

    def send(src, dst, k, device, kr=None):
        copy = pltpu.make_async_remote_copy(
            src_ref=src,
            dst_ref=dst,
            send_sem=ssem.at[k],
            recv_sem=rsem.at[k if kr is None else kr],
            device_id=device,
            device_id_type=MESH,
        )
        copy.start()
        return copy

    def landed(dst, k):
        pltpu.make_async_remote_copy(
            src_ref=dst,
            dst_ref=dst,
            send_sem=ssem.at[k],
            recv_sem=rsem.at[k],
            device_id=partner,
            device_id_type=MESH,
        ).wait_recv()

    streams = (wq_hbm, ck_hbm, cv_hbm, cg_hbm, wo_hbm, wq, ck, cv, cg, wo)
    start_loads(*streams, qs, sc, asem)
    weight_loads = [
        pltpu.make_async_copy(src, dst, wsem.at[i])
        for i, (src, dst) in enumerate(
            (
                (wg_hbm, wg_ref),
                (wu_hbm, wu_ref),
                (ed_hbm, down.at[pl.ds(0, 256)]),
                (dd_hbm, down.at[pl.ds(256, 64)]),
                (dg_hbm, wd.at[pl.ds(0, 64)]),
                (du_hbm, wd.at[pl.ds(128, 64)]),
            )
        )
    ]
    for copy in weight_loads:
        copy.start()

    barrier = pltpu.get_barrier_semaphore()
    for device in (partner, u_plus, u_minus, v_plus, v_minus):
        pl.semaphore_signal(barrier, inc=1, device_id=device, device_id_type=MESH)
    for dz in range(1, 8):
        for core in range(2):
            pl.semaphore_signal(
                barrier, inc=1, device_id=(lax.rem(z + dz, 8), y, x, core), device_id_type=MESH
            )

    table_lane = lax.broadcasted_iota(jnp.int32, (1, EXTRA), 1)
    for s in range(ROWS):
        row = jnp.zeros((1, EXTRA), jnp.float32)
        for choice in range(6):
            row = jnp.where(
                table_lane == ids_ref[choice, s], gw_ref[s] * ew_ref[choice, s], row
            )
        route[s : s + 1, :] = row
    attention(
        inp_ref,
        gain_attn_ref,
        wk_ref,
        wv_ref,
        wf_ref,
        fb_ref,
        len_ref,
        wq_hbm,
        ck_hbm,
        cv_hbm,
        cg_hbm,
        wo_hbm,
        pa_ref,
        wq,
        ck,
        cv,
        cg,
        wo,
        qs,
        sc,
        asem,
    )
    pl.semaphore_wait(barrier, 19)

    sent = []

    sent.append(send(pa_ref, pr, K_PA, partner))
    landed(pr, K_PA)
    attn = pa_ref[...].astype(jnp.float32) + pr[...].astype(jnp.float32)
    after = inp_ref[...].astype(jnp.float32) + attn
    aa[...] = after
    factor = lax.rsqrt(jnp.mean(after * after, axis=-1, keepdims=True) + EPS)
    normed = (after * factor * gain_ref[...].reshape(1, WIDTH)).astype(jnp.bfloat16)

    @pl.when(part == t)
    def _():
        xs[0, v, zz_own, u, :, :WIDTH] = normed
        xs[0, v, zz_own, u, :, WIDTH:] = route[...].astype(jnp.bfloat16)
        block = xs.at[0, v, zz_own, u]
        for dz in (4, 3, 5, 2, 6, 1, 7):
            send(block, block, K_ZG + dz, (lax.rem(z + dz, 8), y, x, t), K_ZG + zz_own)

    vector = vec_ref[...].reshape(1, WIDTH)
    first = vector.astype(jnp.bfloat16).astype(jnp.float32)
    second = (vector - first).astype(jnp.bfloat16).astype(jnp.float32)
    third = vector - first - second
    line = lax.broadcasted_iota(jnp.int32, (ROWS, WIDTH), 0)
    stacked = jnp.where(line == 0, first, jnp.where(line == 1, second, third))
    wd[64:128] = jnp.zeros((64, WIDTH), jnp.bfloat16)
    wd[192:208] = jnp.where(line < 3, stacked, 0.0).astype(jnp.bfloat16)
    wd[208:256] = jnp.zeros((48, WIDTH), jnp.bfloat16)
    down[320:384] = jnp.zeros((64, WIDTH), jnp.bfloat16)
    for copy in weight_loads:
        copy.wait()

    for zz in range(4):

        @pl.when(4 * t + zz != z)
        def _():
            landed(xs.at[0, v, zz, u], K_ZG + zz)

    f32 = jnp.float32
    bf16 = jnp.bfloat16
    right, left, far = mod4(v + 1), mod4(v - 1), mod4(v + 2)
    low, high = pl.ds(0, 2), pl.ds(2, 2)

    def ring_send(piece, w, plus, minus, k):
        own_a, own_b = piece(low, w), piece(high, w)
        sent.append(send(own_a, own_a, k, plus))
        sent.append(send(own_b, own_b, k + 2, minus))
        sent.append(send(own_b, own_b, k + 1, plus))
        sent.append(send(own_a, own_a, k + 3, minus))

    def ring_relay(piece, w, plus, minus, k):
        a_left, b_right = piece(low, mod4(w - 1)), piece(high, mod4(w + 1))
        landed(a_left, k)
        sent.append(send(a_left, a_left, k + 4, plus))
        landed(b_right, k + 2)
        sent.append(send(b_right, b_right, k + 5, minus))

    def piece_u(half, w):
        return xs.at[0, v, half, w]

    def column(n):
        return mod4(u + STAGES[n])

    def piece_v(n):
        return lambda half, w: xs.at[0, w, half, column(n)]

    def push(n, w, slot):
        piece = xs.at[0, w, :, column(n)]
        sent.append(send(piece, xs.at[1, w, :, column(n)], K_PUSH + 4 * n + slot, partner))

    def gather_send(n):
        ring_send(piece_v(n), v, v_plus, v_minus, K_AV + 6 * n)
        push(n, v, 0)

    def gather_relay(n):
        ring_relay(piece_v(n), v, v_plus, v_minus, K_AV + 6 * n)

    def gather_near(n):
        landed(piece_v(n)(high, left), K_AV + 6 * n + 1)
        push(n, left, 1)
        landed(piece_v(n)(low, right), K_AV + 6 * n + 3)
        push(n, right, 2)

    def gather_far(n):
        landed(piece_v(n)(low, far), K_AV + 6 * n + 4)
        landed(piece_v(n)(high, far), K_AV + 6 * n + 5)
        push(n, far, 3)

    lane = lax.broadcasted_iota(jnp.int32, (1, EXTRA), 1)

    def unit(side, col):
        rows = xs[side, :, :, col].reshape(16 * ROWS, ROW)
        tokens = rows[:, :WIDTH]
        weight = jnp.sum(
            jnp.where(lane == expert, rows[:, WIDTH:].astype(f32), 0.0), axis=1, keepdims=True
        )
        gate = jnp.dot(tokens, wg_ref[...], preferred_element_type=f32)
        up = jnp.dot(tokens, wu_ref[...], preferred_element_type=f32)
        hidden = (silu(gate) * up * weight).astype(bf16)
        both = lax.dot_general(
            tokens, wd[...], (((1,), (1,)), ((), ())), preferred_element_type=f32
        )
        second_half = both[:, EXTRA:]
        logit = jnp.sum(
            jnp.where((lane >= 64) & (lane < 67), second_half, 0.0), axis=1, keepdims=True
        )
        gating = 1.0 / (1.0 + jnp.exp(-logit))
        dense = (silu(both[:, :EXTRA]) * second_half * gating).astype(bf16)
        hidden = jnp.concatenate([hidden, dense], axis=1)
        total = jnp.dot(hidden, down[...], preferred_element_type=f32).astype(bf16)
        po[side, :, :, col] = total.reshape(4, 4, ROWS, WIDTH)

    def own_unit(n):
        unit(0, column(n))

    def partner_unit(n):
        col = mod4(v + STAGES[n])
        for slot, step in enumerate((0, -1, 1, 2)):
            landed(xs.at[1, mod4(u + step), :, col], K_PUSH + 4 * n + slot)
        unit(1, col)
        sent.append(send(po.at[1, :, :, col], dr.at[:, :, col], K_PART + n, partner))

    def add_into(target, source, count):
        for i in range(count):
            target[i] = (target[i].astype(f32) + source[i].astype(f32)).astype(bf16)

    def reduce_send(n):
        col = column(n)
        k = K_RV + 6 * n
        landed(dr.at[:, :, col], K_PART + n)

        def take(w):
            add_into(po.at[0, w, :, col], dr.at[w, :, col], 4)

        take(far)
        sent.append(send(po.at[0, far, low, col], va.at[col], k, v_plus))
        sent.append(send(po.at[0, far, high, col], vb.at[col], k + 1, v_minus))
        take(right)
        sent.append(send(po.at[0, right, high, col], vf.at[1, col], k + 2, v_plus))
        take(left)
        sent.append(send(po.at[0, left, low, col], vf.at[0, col], k + 3, v_minus))

    def reduce_relay(n):
        col = column(n)
        k = K_RV + 6 * n
        landed(va.at[col], k)
        add_into(po.at[0, right, low, col], va.at[col], 2)
        sent.append(send(po.at[0, right, low, col], vf.at[2, col], k + 4, v_plus))
        landed(vb.at[col], k + 1)
        add_into(po.at[0, left, high, col], vb.at[col], 2)
        sent.append(send(po.at[0, left, high, col], vf.at[3, col], k + 5, v_minus))

    def reduce_end(n):
        col = column(n)
        k = K_RV + 6 * n
        landed(vf.at[0, col], k + 3)
        landed(vf.at[1, col], k + 2)
        landed(vf.at[2, col], k + 4)
        landed(vf.at[3, col], k + 5)
        for zz in range(4):
            half, inner = zz // 2, zz % 2
            total = (
                po[0, v, zz, col].astype(f32)
                + dr[v, zz, col].astype(f32)
                + vf[half, col, inner].astype(f32)
                + vf[2 + half, col, inner].astype(f32)
            )
            sv[col, zz] = total.astype(bf16)

    up_col, far_col, down_col = column(1), column(2), column(3)
    ring_send(piece_u, u, u_plus, u_minus, K_AU)
    gather_send(0)
    ring_relay(piece_u, u, u_plus, u_minus, K_AU)
    landed(piece_u(low, mod4(u + 1)), K_AU + 3)
    landed(piece_u(high, mod4(u - 1)), K_AU + 1)
    gather_send(1)
    gather_relay(0)
    landed(piece_u(low, mod4(u + 2)), K_AU + 4)
    landed(piece_u(high, mod4(u + 2)), K_AU + 5)
    gather_relay(1)
    gather_near(0)
    gather_send(2)
    gather_near(1)
    gather_send(3)
    gather_far(0)
    own_unit(0)
    gather_far(1)
    partner_unit(0)
    gather_relay(2)
    own_unit(1)
    gather_near(2)
    gather_relay(3)
    partner_unit(1)
    reduce_send(0)
    gather_far(2)
    gather_near(3)
    own_unit(2)
    gather_far(3)
    partner_unit(2)
    reduce_send(1)
    partner_unit(3)
    reduce_send(2)
    own_unit(3)
    reduce_send(3)
    reduce_relay(2)
    reduce_relay(1)
    reduce_relay(3)
    reduce_end(2)
    sent.append(send(sv.at[far_col, low], ua, K_RU, u_plus))
    sent.append(send(sv.at[far_col, high], ub, K_RU + 1, u_minus))
    reduce_relay(0)
    reduce_end(1)
    reduce_end(3)
    sent.append(send(sv.at[down_col, low], uf.at[0], K_RU + 3, u_minus))
    sent.append(send(sv.at[up_col, high], uf.at[1], K_RU + 2, u_plus))
    landed(ua, K_RU)
    add_into(sv.at[up_col, low], ua, 2)
    sent.append(send(sv.at[up_col, low], uf.at[2], K_RU + 4, u_plus))
    landed(ub, K_RU + 1)
    add_into(sv.at[down_col, high], ub, 2)
    sent.append(send(sv.at[down_col, high], uf.at[3], K_RU + 5, u_minus))
    reduce_end(0)
    for half in range(2):
        landed(uf.at[half], K_RU + 3 - half)
        landed(uf.at[2 + half], K_RU + 4 + half)
        for inner in range(2):
            zz = 2 * half + inner
            total = (
                sv[u, zz].astype(f32)
                + uf[half, inner].astype(f32)
                + uf[2 + half, inner].astype(f32)
            ).astype(bf16)
            for h in range(2):
                su[zz, h] = total[:, h * HALF : (h + 1) * HALF]
                here = (4 * t + zz == z) & (t == h)

                @pl.when(jnp.logical_not(here))
                def _():
                    send(
                        su.at[zz, h],
                        zr.at[z],
                        K_ZR + zz * 2 + h,
                        (4 * t + zz, y, x, h),
                        K_ZR + z,
                    )

                @pl.when(here)
                def _():
                    zr[z] = su[zz, h]

    for s in range(8):

        @pl.when(jnp.logical_not((z == s) & (part == t)))
        def _():
            landed(zr.at[s], K_ZR + s)

    total = aa[:, pl.ds(pl.multiple_of(t * HALF, HALF), HALF)]
    for s in range(8):
        total = total + zr[s].astype(f32)
    out_ref[...] = total.astype(bf16)

    for copy in sent:
        copy.wait_send()

    def sent_out(src, k):
        pltpu.make_async_remote_copy(
            src_ref=src,
            dst_ref=src,
            send_sem=ssem.at[k],
            recv_sem=rsem.at[k],
            device_id=partner,
            device_id_type=MESH,
        ).wait_send()

    @pl.when(part == t)
    def _():
        for dz in range(1, 8):
            sent_out(xs.at[0, v, zz_own, u], K_ZG + dz)

    for zz in range(4):
        for h in range(2):

            @pl.when(jnp.logical_not((4 * t + zz == z) & (t == h)))
            def _():
                sent_out(su.at[zz, h], K_ZR + zz * 2 + h)


def run_layer(*arrays):
    bf16 = jnp.bfloat16
    vmem = pl.BlockSpec(memory_space=pltpu.VMEM)
    smem = pl.BlockSpec(memory_space=pltpu.SMEM)
    hbm = pl.BlockSpec(memory_space=pltpu.HBM)
    return pl.pallas_call(
        layer_kernel,
        out_shape=jax.ShapeDtypeStruct((ROWS, HALF), bf16),
        in_specs=[vmem] * 5
        + [smem] * 2
        + [hbm] * 5
        + [vmem]
        + [smem] * 3
        + [hbm] * 3
        + [vmem]
        + [hbm] * 3,
        out_specs=vmem,
        scratch_shapes=[
            pltpu.VMEM((WIDTH, 256), bf16),
            pltpu.VMEM((WIDTH, 256), bf16),
            pltpu.VMEM((ROWS, WIDTH), bf16),
            pltpu.VMEM((ROWS, EXTRA), jnp.float32),
            pltpu.SemaphoreType.DMA((6,)),
            *att_scratch(),
            pltpu.VMEM((256, WIDTH), bf16),
            pltpu.VMEM((384, WIDTH), bf16),
            pltpu.VMEM((ROWS, WIDTH), bf16),
            pltpu.VMEM((ROWS, WIDTH), jnp.float32),
            pltpu.VMEM((2, 4, 4, 4, ROWS, ROW), bf16),
            pltpu.VMEM((2, 4, 4, 4, ROWS, WIDTH), bf16),
            pltpu.VMEM((4, 4, 4, ROWS, WIDTH), bf16),
            pltpu.VMEM((4, 2, ROWS, WIDTH), bf16),
            pltpu.VMEM((4, 2, ROWS, WIDTH), bf16),
            pltpu.VMEM((4, 4, 2, ROWS, WIDTH), bf16),
            pltpu.VMEM((4, 4, ROWS, WIDTH), bf16),
            pltpu.VMEM((2, ROWS, WIDTH), bf16),
            pltpu.VMEM((2, ROWS, WIDTH), bf16),
            pltpu.VMEM((4, 2, ROWS, WIDTH), bf16),
            pltpu.VMEM((4, 2, ROWS, HALF), bf16),
            pltpu.VMEM((8, ROWS, HALF), bf16),
            pltpu.SemaphoreType.DMA((N_SEM,)),
            pltpu.SemaphoreType.DMA((N_SEM,)),
        ],
        compiler_params=pltpu.CompilerParams(
            collective_id=0, has_side_effects=True, vmem_limit_bytes=60 * 1024 * 1024
        ),
        name="layer",
    )(*arrays)


def shards(
    inputs,
    norm_gain_attn,
    w_query,
    w_key,
    w_value,
    w_forget,
    forget_bias,
    cache_keys,
    cache_values,
    cache_gates,
    lengths,
    w_out,
    norm_gain_ffn,
    expert_ids,
    group_weights,
    expert_weights,
    exp_gate,
    exp_up,
    exp_down,
    dense_gate_vector,
    dense_gate_w,
    dense_up_w,
    dense_down_w,
):
    return run_layer(
        inputs,
        norm_gain_attn,
        w_key.T,
        w_value.T,
        w_forget.T,
        forget_bias,
        lengths,
        w_query,
        cache_keys[:, 0].transpose(0, 2, 1),
        cache_values[:, 0].transpose(0, 2, 1),
        cache_gates.transpose(1, 0, 2),
        w_out,
        norm_gain_ffn,
        expert_ids.T,
        group_weights,
        expert_weights.T,
        exp_gate[0],
        exp_up[0],
        exp_down[0],
        dense_gate_vector,
        dense_gate_w.T,
        dense_up_w.T,
        dense_down_w,
    )


def solution(mesh):
    torus = Mesh(mesh.devices.reshape(8, 4, 4, mesh.shape["tp"]), ("ep_0", "ep_1", "ep_2", "tp"))
    placed = (
        P(EP, None),
        P(),
        P(None, "tp"),
        P(None, "tp"),
        P(None, "tp"),
        P(None, "tp"),
        P("tp"),
        P(EP, "tp", None, None),
        P(EP, "tp", None, None),
        P(EP, "tp", None),
        P(EP),
        P("tp", None),
        P(),
        P(EP, None),
        P(EP),
        P(EP, None),
        P(EP, None, "tp"),
        P(EP, None, "tp"),
        P(EP, "tp", None),
        P(),
        P(None, EP_TP),
        P(None, EP_TP),
        P(EP_TP, None),
    )
    return jax.shard_map(
        shards, mesh=torus, in_specs=placed, out_specs=P(EP, "tp"), check_vma=False
    )
```

```python
import jax
import jax.numpy as jnp
from jax import lax
from jax.experimental import pallas as pl
from jax.experimental.pallas import tpu as pltpu
from jax.sharding import Mesh
from jax.sharding import PartitionSpec as P

EP = ("ep_0", "ep_1", "ep_2")
EP_TP = ("ep_0", "ep_1", "ep_2", "tp")


EPS = 1e-06


MESH = pl.DeviceIdType.MESH
WIDTH = 1536
HALF = WIDTH // 2
EXTRA = 128
ROW = WIDTH + EXTRA
ROWS = 16

K_PA = 0
K_ZG = 1
K_AU = 9
K_ZR = 15
K_RU = 23
K_AV = 29
K_PUSH = 53
K_PART = 69
K_RV = 73
N_SEM = 97

STAGES = (0, 1, 2, -1)


def mod4(value):
    return lax.rem(value + 8, 4)


def silu(value):
    return value / (1.0 + jnp.exp(-value))


def att_scratch():
    bf16, f32 = jnp.bfloat16, jnp.float32
    return [
        pltpu.VMEM((1536, 384), bf16),
        pltpu.VMEM((16, 64, 1024), bf16),
        pltpu.VMEM((16, 64, 1024), bf16),
        pltpu.VMEM((6, 16, 1024), f32),
        pltpu.VMEM((384, 1536), bf16),
        pltpu.VMEM((128, 128), f32),
        pltpu.VMEM((1024, 128), f32),
        pltpu.SemaphoreType.DMA((8,)),
    ]


def att_copies(wq_hbm, ck_hbm, cv_hbm, cg_hbm, wo_hbm, wq, ck, cv, cg, wo, sem):
    half = pl.ds(0, 8), pl.ds(8, 8)
    pairs = [
        (wq_hbm, wq),
        (ck_hbm.at[half[0]], ck.at[half[0]]),
        (ck_hbm.at[half[1]], ck.at[half[1]]),
        (cg_hbm, cg),
        (cv_hbm.at[half[0]], cv.at[half[0]]),
        (cv_hbm.at[half[1]], cv.at[half[1]]),
        (wo_hbm, wo),
    ]
    return [pltpu.make_async_copy(src, dst, sem.at[i]) for i, (src, dst) in enumerate(pairs)]


def start_loads(wq_hbm, ck_hbm, cv_hbm, cg_hbm, wo_hbm, wq, ck, cv, cg, wo, qs, sc, sem):
    for copy in att_copies(wq_hbm, ck_hbm, cv_hbm, cg_hbm, wo_hbm, wq, ck, cv, cg, wo, sem):
        copy.start()


def attention(
    inp_ref,
    gain_ref,
    wk_ref,
    wv_ref,
    wf_ref,
    fb_ref,
    len_ref,
    wq_hbm,
    ck_hbm,
    cv_hbm,
    cg_hbm,
    wo_hbm,
    out_ref,
    wq,
    ck,
    cv,
    cg,
    wo,
    qs,
    sc,
    sem,
):
    f32, bf16 = jnp.float32, jnp.bfloat16
    loads = att_copies(wq_hbm, ck_hbm, cv_hbm, cg_hbm, wo_hbm, wq, ck, cv, cg, wo, sem)
    transposed = (((1,), (1,)), ((), ()))
    row_block = inp_ref[...].astype(f32)
    factor = lax.rsqrt(jnp.mean(row_block * row_block, axis=-1, keepdims=True) + EPS)
    normed = (row_block * factor * gain_ref[...].reshape(1, WIDTH)).astype(bf16)
    new_key = lax.dot_general(normed, wk_ref[...], transposed, preferred_element_type=f32)
    new_key = new_key.astype(bf16).astype(f32)
    new_value = lax.dot_general(normed, wv_ref[...], transposed, preferred_element_type=f32)
    new_value = new_value.astype(bf16).astype(f32)
    logit = lax.dot_general(normed, wf_ref[...], transposed, preferred_element_type=f32)
    loads[0].wait()
    queries = jnp.dot(normed, wq[...], preferred_element_type=f32).astype(bf16).astype(f32)
    own_scores = []
    qs[...] = jnp.zeros((128, 128), f32)

    def head_rows(h):
        return pl.ds(h, 16, stride=8)

    def load_head(h):
        return jnp.concatenate(
            [sc[pl.ds(128 * c + h, 16, stride=8), :] for c in range(8)], axis=1
        )

    for h in range(6):
        query = queries[:, 128 * (h // 2) : 128 * (h // 2) + 128]
        if h % 2:
            query = pltpu.roll(query, 64, 1)
        own_scores.append(jnp.sum(query[:, :64] * new_key, axis=1, keepdims=True) * 0.125)
        qs[head_rows(h), :] = query
    for s in range(16):
        if s % 8 == 0:
            loads[1 + s // 8].wait()
        scores = jnp.dot(
            qs[8 * s : 8 * s + 8, :64].astype(bf16), ck[s], preferred_element_type=f32
        )
        for c in range(8):
            sc[128 * c + 8 * s : 128 * c + 8 * s + 8, :] = scores[:, 128 * c : 128 * c + 128]
    loads[3].wait()
    line = lax.broadcasted_iota(jnp.int32, (16, 1), 0)
    counts = jnp.zeros((16, 1), jnp.int32)
    for s in range(16):
        counts = jnp.where(line == s, len_ref[s], counts)
    positions = lax.broadcasted_iota(jnp.int32, (16, 1024), 1)
    valid = positions < counts
    newest = positions == counts - 1
    own_weights = []
    for h in range(6):
        gates = cg[h]
        last = jnp.sum(jnp.where(newest, gates, 0.0), axis=1, keepdims=True)
        forget = logit[:, h : h + 1] + fb_ref[h]
        forget = jnp.minimum(forget, 0.0) - jnp.log1p(jnp.exp(-jnp.abs(forget)))
        offsets = (last + forget) - gates
        cached = load_head(h) * 0.125 + offsets
        cached = jnp.where(valid, cached, -jnp.inf)
        own = own_scores[h]
        peak = jnp.maximum(jnp.max(cached, axis=1, keepdims=True), own)
        cached = jnp.exp(cached - peak)
        own = jnp.exp(own - peak)
        denominator = jnp.sum(cached, axis=1, keepdims=True) + own
        cached = cached / denominator
        for c in range(8):
            sc[pl.ds(128 * c + h, 16, stride=8), :] = cached[:, 128 * c : 128 * c + 128]
        own_weights.append((own / denominator).astype(bf16).astype(f32))
    for s in range(16):
        if s % 8 == 0:
            loads[4 + s // 8].wait()
        weights = jnp.concatenate(
            [sc[128 * c + 8 * s : 128 * c + 8 * s + 8, :] for c in range(8)], axis=1
        )
        qs[8 * s : 8 * s + 8, :64] = lax.dot_general(
            weights.astype(bf16), cv[s], transposed, preferred_element_type=f32
        )
    loads[6].wait()
    total = jnp.zeros((16, 1536), f32)
    for h in range(6):
        head = qs[head_rows(h), :][:, :64] + own_weights[h] * new_value
        total = total + jnp.dot(
            head.astype(bf16), wo[64 * h : 64 * h + 64, :], preferred_element_type=f32
        )
    out_ref[...] = total.astype(bf16)


def layer_kernel(
    inp_ref,
    gain_attn_ref,
    wk_ref,
    wv_ref,
    wf_ref,
    fb_ref,
    len_ref,
    wq_hbm,
    ck_hbm,
    cv_hbm,
    cg_hbm,
    wo_hbm,
    gain_ref,
    ids_ref,
    gw_ref,
    ew_ref,
    wg_hbm,
    wu_hbm,
    ed_hbm,
    vec_ref,
    dg_hbm,
    du_hbm,
    dd_hbm,
    out_ref,
    wg_ref,
    wu_ref,
    pa_ref,
    route,
    wsem,
    wq,
    ck,
    cv,
    cg,
    wo,
    qs,
    sc,
    asem,
    wd,
    down,
    pr,
    aa,
    xs,
    po,
    dr,
    va,
    vb,
    vf,
    sv,
    ua,
    ub,
    uf,
    su,
    zr,
    ssem,
    rsem,
):
    z = lax.axis_index("ep_0")
    y = lax.axis_index("ep_1")
    x = lax.axis_index("ep_2")
    t = lax.axis_index("tp")
    expert = (z * 4 + y) * 4 + x
    u = (1 - t) * y + t * x
    v = (1 - t) * x + t * y
    part = z // 4
    zz_own = lax.rem(z, 4)

    def near(du, dv):
        return (z, mod4(y + (1 - t) * du + t * dv), mod4(x + (1 - t) * dv + t * du), t)

    partner = (z, y, x, 1 - t)
    u_plus, u_minus = near(1, 0), near(-1, 0)
    v_plus, v_minus = near(0, 1), near(0, -1)

    def send(src, dst, k, device, kr=None):
        copy = pltpu.make_async_remote_copy(
            src_ref=src,
            dst_ref=dst,
            send_sem=ssem.at[k],
            recv_sem=rsem.at[k if kr is None else kr],
            device_id=device,
            device_id_type=MESH,
        )
        copy.start()
        return copy

    def landed(dst, k):
        pltpu.make_async_remote_copy(
            src_ref=dst,
            dst_ref=dst,
            send_sem=ssem.at[k],
            recv_sem=rsem.at[k],
            device_id=partner,
            device_id_type=MESH,
        ).wait_recv()

    streams = (wq_hbm, ck_hbm, cv_hbm, cg_hbm, wo_hbm, wq, ck, cv, cg, wo)
    start_loads(*streams, qs, sc, asem)
    weight_loads = [
        pltpu.make_async_copy(src, dst, wsem.at[i])
        for i, (src, dst) in enumerate(
            (
                (wg_hbm, wg_ref),
                (wu_hbm, wu_ref),
                (ed_hbm, down.at[pl.ds(0, 256)]),
                (dd_hbm, down.at[pl.ds(256, 64)]),
                (dg_hbm, wd.at[pl.ds(0, 64)]),
                (du_hbm, wd.at[pl.ds(128, 64)]),
            )
        )
    ]
    for copy in weight_loads:
        copy.start()

    barrier = pltpu.get_barrier_semaphore()
    for device in (partner, u_plus, u_minus, v_plus, v_minus):
        pl.semaphore_signal(barrier, inc=1, device_id=device, device_id_type=MESH)
    for dz in range(1, 8):
        for core in range(2):
            pl.semaphore_signal(
                barrier, inc=1, device_id=(lax.rem(z + dz, 8), y, x, core), device_id_type=MESH
            )

    table_lane = lax.broadcasted_iota(jnp.int32, (1, EXTRA), 1)
    for s in range(ROWS):
        row = jnp.zeros((1, EXTRA), jnp.float32)
        for choice in range(6):
            row = jnp.where(
                table_lane == ids_ref[choice, s], gw_ref[s] * ew_ref[choice, s], row
            )
        route[s : s + 1, :] = row
    attention(
        inp_ref,
        gain_attn_ref,
        wk_ref,
        wv_ref,
        wf_ref,
        fb_ref,
        len_ref,
        wq_hbm,
        ck_hbm,
        cv_hbm,
        cg_hbm,
        wo_hbm,
        pa_ref,
        wq,
        ck,
        cv,
        cg,
        wo,
        qs,
        sc,
        asem,
    )
    pl.semaphore_wait(barrier, 19)

    sent = []

    sent.append(send(pa_ref, pr, K_PA, partner))
    landed(pr, K_PA)
    attn = pa_ref[...].astype(jnp.float32) + pr[...].astype(jnp.float32)
    after = inp_ref[...].astype(jnp.float32) + attn
    aa[...] = after
    factor = lax.rsqrt(jnp.mean(after * after, axis=-1, keepdims=True) + EPS)
    normed = (after * factor * gain_ref[...].reshape(1, WIDTH)).astype(jnp.bfloat16)

    @pl.when(part == t)
    def _():
        xs[0, v, zz_own, u, :, :WIDTH] = normed
        xs[0, v, zz_own, u, :, WIDTH:] = route[...].astype(jnp.bfloat16)
        block = xs.at[0, v, zz_own, u]
        for dz in (4, 3, 5, 2, 6, 1, 7):
            send(block, block, K_ZG + dz, (lax.rem(z + dz, 8), y, x, t), K_ZG + zz_own)

    vector = vec_ref[...].reshape(1, WIDTH)
    first = vector.astype(jnp.bfloat16).astype(jnp.float32)
    second = (vector - first).astype(jnp.bfloat16).astype(jnp.float32)
    third = vector - first - second
    line = lax.broadcasted_iota(jnp.int32, (ROWS, WIDTH), 0)
    stacked = jnp.where(line == 0, first, jnp.where(line == 1, second, third))
    wd[64:128] = jnp.zeros((64, WIDTH), jnp.bfloat16)
    wd[192:208] = jnp.where(line < 3, stacked, 0.0).astype(jnp.bfloat16)
    wd[208:256] = jnp.zeros((48, WIDTH), jnp.bfloat16)
    down[320:384] = jnp.zeros((64, WIDTH), jnp.bfloat16)
    for copy in weight_loads:
        copy.wait()

    for zz in range(4):

        @pl.when(4 * t + zz != z)
        def _():
            landed(xs.at[0, v, zz, u], K_ZG + zz)

    f32 = jnp.float32
    bf16 = jnp.bfloat16
    right, left, far = mod4(v + 1), mod4(v - 1), mod4(v + 2)
    low, high = pl.ds(0, 2), pl.ds(2, 2)

    def ring_send(piece, w, plus, minus, k):
        own_a, own_b = piece(low, w), piece(high, w)
        sent.append(send(own_a, own_a, k, plus))
        sent.append(send(own_b, own_b, k + 2, minus))
        sent.append(send(own_b, own_b, k + 1, plus))
        sent.append(send(own_a, own_a, k + 3, minus))

    def ring_relay(piece, w, plus, minus, k):
        a_left, b_right = piece(low, mod4(w - 1)), piece(high, mod4(w + 1))
        landed(a_left, k)
        sent.append(send(a_left, a_left, k + 4, plus))
        landed(b_right, k + 2)
        sent.append(send(b_right, b_right, k + 5, minus))

    def piece_u(half, w):
        return xs.at[0, v, half, w]

    def column(n):
        return mod4(u + STAGES[n])

    def piece_v(n):
        return lambda half, w: xs.at[0, w, half, column(n)]

    def push(n, w, slot):
        piece = xs.at[0, w, :, column(n)]
        sent.append(send(piece, xs.at[1, w, :, column(n)], K_PUSH + 4 * n + slot, partner))

    def gather_send(n):
        ring_send(piece_v(n), v, v_plus, v_minus, K_AV + 6 * n)
        push(n, v, 0)

    def gather_relay(n):
        ring_relay(piece_v(n), v, v_plus, v_minus, K_AV + 6 * n)

    def gather_near(n):
        landed(piece_v(n)(high, left), K_AV + 6 * n + 1)
        push(n, left, 1)
        landed(piece_v(n)(low, right), K_AV + 6 * n + 3)
        push(n, right, 2)

    def gather_far(n):
        landed(piece_v(n)(low, far), K_AV + 6 * n + 4)
        landed(piece_v(n)(high, far), K_AV + 6 * n + 5)
        push(n, far, 3)

    lane = lax.broadcasted_iota(jnp.int32, (1, EXTRA), 1)

    def unit(side, col):
        rows = xs[side, :, :, col].reshape(16 * ROWS, ROW)
        tokens = rows[:, :WIDTH]
        weight = jnp.sum(
            jnp.where(lane == expert, rows[:, WIDTH:].astype(f32), 0.0), axis=1, keepdims=True
        )
        gate = jnp.dot(tokens, wg_ref[...], preferred_element_type=f32)
        up = jnp.dot(tokens, wu_ref[...], preferred_element_type=f32)
        hidden = (silu(gate) * up * weight).astype(bf16)
        both = lax.dot_general(
            tokens, wd[...], (((1,), (1,)), ((), ())), preferred_element_type=f32
        )
        second_half = both[:, EXTRA:]
        logit = jnp.sum(
            jnp.where((lane >= 64) & (lane < 67), second_half, 0.0), axis=1, keepdims=True
        )
        gating = 1.0 / (1.0 + jnp.exp(-logit))
        dense = (silu(both[:, :EXTRA]) * second_half * gating).astype(bf16)
        hidden = jnp.concatenate([hidden, dense], axis=1)
        total = jnp.dot(hidden, down[...], preferred_element_type=f32).astype(bf16)
        po[side, :, :, col] = total.reshape(4, 4, ROWS, WIDTH)

    def own_unit(n):
        unit(0, column(n))

    def partner_unit(n):
        col = mod4(v + STAGES[n])
        for slot, step in enumerate((0, -1, 1, 2)):
            landed(xs.at[1, mod4(u + step), :, col], K_PUSH + 4 * n + slot)
        unit(1, col)
        sent.append(send(po.at[1, :, :, col], dr.at[:, :, col], K_PART + n, partner))

    def add_into(target, source, count):
        for i in range(count):
            target[i] = (target[i].astype(f32) + source[i].astype(f32)).astype(bf16)

    def reduce_send(n):
        col = column(n)
        k = K_RV + 6 * n
        landed(dr.at[:, :, col], K_PART + n)

        def take(w):
            add_into(po.at[0, w, :, col], dr.at[w, :, col], 4)

        take(far)
        sent.append(send(po.at[0, far, low, col], va.at[col], k, v_plus))
        sent.append(send(po.at[0, far, high, col], vb.at[col], k + 1, v_minus))
        take(right)
        sent.append(send(po.at[0, right, high, col], vf.at[1, col], k + 2, v_plus))
        take(left)
        sent.append(send(po.at[0, left, low, col], vf.at[0, col], k + 3, v_minus))

    def reduce_relay(n):
        col = column(n)
        k = K_RV + 6 * n
        landed(va.at[col], k)
        add_into(po.at[0, right, low, col], va.at[col], 2)
        sent.append(send(po.at[0, right, low, col], vf.at[2, col], k + 4, v_plus))
        landed(vb.at[col], k + 1)
        add_into(po.at[0, left, high, col], vb.at[col], 2)
        sent.append(send(po.at[0, left, high, col], vf.at[3, col], k + 5, v_minus))

    def reduce_end(n):
        col = column(n)
        k = K_RV + 6 * n
        landed(vf.at[0, col], k + 3)
        landed(vf.at[1, col], k + 2)
        landed(vf.at[2, col], k + 4)
        landed(vf.at[3, col], k + 5)
        for zz in range(4):
            half, inner = zz // 2, zz % 2
            total = (
                po[0, v, zz, col].astype(f32)
                + dr[v, zz, col].astype(f32)
                + vf[half, col, inner].astype(f32)
                + vf[2 + half, col, inner].astype(f32)
            )
            sv[col, zz] = total.astype(bf16)

    up_col, far_col, down_col = column(1), column(2), column(3)
    ring_send(piece_u, u, u_plus, u_minus, K_AU)
    gather_send(0)
    ring_relay(piece_u, u, u_plus, u_minus, K_AU)
    landed(piece_u(low, mod4(u + 1)), K_AU + 3)
    landed(piece_u(high, mod4(u - 1)), K_AU + 1)
    gather_send(3)
    gather_relay(0)
    gather_near(0)
    landed(piece_u(low, mod4(u + 2)), K_AU + 4)
    landed(piece_u(high, mod4(u + 2)), K_AU + 5)
    gather_relay(3)
    gather_near(3)
    gather_send(2)
    gather_send(1)
    gather_far(0)
    own_unit(0)
    gather_far(3)
    partner_unit(0)
    gather_relay(2)
    partner_unit(3)
    gather_relay(1)
    own_unit(3)
    gather_near(2)
    reduce_send(0)
    gather_far(2)
    own_unit(2)
    gather_near(1)
    reduce_send(3)
    gather_far(1)
    partner_unit(2)
    reduce_relay(0)
    partner_unit(1)
    reduce_send(2)
    own_unit(1)
    reduce_send(1)
    reduce_relay(2)
    reduce_relay(3)
    reduce_relay(1)
    reduce_end(2)
    sent.append(send(sv.at[far_col, low], ua, K_RU, u_plus))
    sent.append(send(sv.at[far_col, high], ub, K_RU + 1, u_minus))
    reduce_end(3)
    reduce_end(0)
    reduce_end(1)
    sent.append(send(sv.at[up_col, high], uf.at[1], K_RU + 2, u_plus))
    sent.append(send(sv.at[down_col, low], uf.at[0], K_RU + 3, u_minus))
    landed(ua, K_RU)
    add_into(sv.at[up_col, low], ua, 2)
    sent.append(send(sv.at[up_col, low], uf.at[2], K_RU + 4, u_plus))
    landed(ub, K_RU + 1)
    add_into(sv.at[down_col, high], ub, 2)
    sent.append(send(sv.at[down_col, high], uf.at[3], K_RU + 5, u_minus))
    for half in range(2):
        landed(uf.at[half], K_RU + 3 - half)
        landed(uf.at[2 + half], K_RU + 4 + half)
        for inner in range(2):
            zz = 2 * half + inner
            total = (
                sv[u, zz].astype(f32)
                + uf[half, inner].astype(f32)
                + uf[2 + half, inner].astype(f32)
            ).astype(bf16)
            for h in range(2):
                su[zz, h] = total[:, h * HALF : (h + 1) * HALF]
                here = (4 * t + zz == z) & (t == h)

                @pl.when(jnp.logical_not(here))
                def _():
                    send(
                        su.at[zz, h],
                        zr.at[z],
                        K_ZR + zz * 2 + h,
                        (4 * t + zz, y, x, h),
                        K_ZR + z,
                    )

                @pl.when(here)
                def _():
                    zr[z] = su[zz, h]

    for s in range(8):

        @pl.when(jnp.logical_not((z == s) & (part == t)))
        def _():
            landed(zr.at[s], K_ZR + s)

    total = aa[:, pl.ds(pl.multiple_of(t * HALF, HALF), HALF)]
    for s in range(8):
        total = total + zr[s].astype(f32)
    out_ref[...] = total.astype(bf16)

    for copy in sent:
        copy.wait_send()

    def sent_out(src, k):
        pltpu.make_async_remote_copy(
            src_ref=src,
            dst_ref=src,
            send_sem=ssem.at[k],
            recv_sem=rsem.at[k],
            device_id=partner,
            device_id_type=MESH,
        ).wait_send()

    @pl.when(part == t)
    def _():
        for dz in range(1, 8):
            sent_out(xs.at[0, v, zz_own, u], K_ZG + dz)

    for zz in range(4):
        for h in range(2):

            @pl.when(jnp.logical_not((4 * t + zz == z) & (t == h)))
            def _():
                sent_out(su.at[zz, h], K_ZR + zz * 2 + h)


def run_layer(*arrays):
    bf16 = jnp.bfloat16
    vmem = pl.BlockSpec(memory_space=pltpu.VMEM)
    smem = pl.BlockSpec(memory_space=pltpu.SMEM)
    hbm = pl.BlockSpec(memory_space=pltpu.HBM)
    return pl.pallas_call(
        layer_kernel,
        out_shape=jax.ShapeDtypeStruct((ROWS, HALF), bf16),
        in_specs=[vmem] * 5
        + [smem] * 2
        + [hbm] * 5
        + [vmem]
        + [smem] * 3
        + [hbm] * 3
        + [vmem]
        + [hbm] * 3,
        out_specs=vmem,
        scratch_shapes=[
            pltpu.VMEM((WIDTH, 256), bf16),
            pltpu.VMEM((WIDTH, 256), bf16),
            pltpu.VMEM((ROWS, WIDTH), bf16),
            pltpu.VMEM((ROWS, EXTRA), jnp.float32),
            pltpu.SemaphoreType.DMA((6,)),
            *att_scratch(),
            pltpu.VMEM((256, WIDTH), bf16),
            pltpu.VMEM((384, WIDTH), bf16),
            pltpu.VMEM((ROWS, WIDTH), bf16),
            pltpu.VMEM((ROWS, WIDTH), jnp.float32),
            pltpu.VMEM((2, 4, 4, 4, ROWS, ROW), bf16),
            pltpu.VMEM((2, 4, 4, 4, ROWS, WIDTH), bf16),
            pltpu.VMEM((4, 4, 4, ROWS, WIDTH), bf16),
            pltpu.VMEM((4, 2, ROWS, WIDTH), bf16),
            pltpu.VMEM((4, 2, ROWS, WIDTH), bf16),
            pltpu.VMEM((4, 4, 2, ROWS, WIDTH), bf16),
            pltpu.VMEM((4, 4, ROWS, WIDTH), bf16),
            pltpu.VMEM((2, ROWS, WIDTH), bf16),
            pltpu.VMEM((2, ROWS, WIDTH), bf16),
            pltpu.VMEM((4, 2, ROWS, WIDTH), bf16),
            pltpu.VMEM((4, 2, ROWS, HALF), bf16),
            pltpu.VMEM((8, ROWS, HALF), bf16),
            pltpu.SemaphoreType.DMA((N_SEM,)),
            pltpu.SemaphoreType.DMA((N_SEM,)),
        ],
        compiler_params=pltpu.CompilerParams(
            collective_id=0, has_side_effects=True, vmem_limit_bytes=60 * 1024 * 1024
        ),
        name="layer",
    )(*arrays)


def shards(
    inputs,
    norm_gain_attn,
    w_query,
    w_key,
    w_value,
    w_forget,
    forget_bias,
    cache_keys,
    cache_values,
    cache_gates,
    lengths,
    w_out,
    norm_gain_ffn,
    expert_ids,
    group_weights,
    expert_weights,
    exp_gate,
    exp_up,
    exp_down,
    dense_gate_vector,
    dense_gate_w,
    dense_up_w,
    dense_down_w,
):
    return run_layer(
        inputs,
        norm_gain_attn,
        w_key.T,
        w_value.T,
        w_forget.T,
        forget_bias,
        lengths,
        w_query,
        cache_keys[:, 0].transpose(0, 2, 1),
        cache_values[:, 0].transpose(0, 2, 1),
        cache_gates.transpose(1, 0, 2),
        w_out,
        norm_gain_ffn,
        expert_ids.T,
        group_weights,
        expert_weights.T,
        exp_gate[0],
        exp_up[0],
        exp_down[0],
        dense_gate_vector,
        dense_gate_w.T,
        dense_up_w.T,
        dense_down_w,
    )


def solution(mesh):
    torus = Mesh(mesh.devices.reshape(8, 4, 4, mesh.shape["tp"]), ("ep_0", "ep_1", "ep_2", "tp"))
    placed = (
        P(EP, None),
        P(),
        P(None, "tp"),
        P(None, "tp"),
        P(None, "tp"),
        P(None, "tp"),
        P("tp"),
        P(EP, "tp", None, None),
        P(EP, "tp", None, None),
        P(EP, "tp", None),
        P(EP),
        P("tp", None),
        P(),
        P(EP, None),
        P(EP),
        P(EP, None),
        P(EP, None, "tp"),
        P(EP, None, "tp"),
        P(EP, "tp", None),
        P(),
        P(None, EP_TP),
        P(None, EP_TP),
        P(EP_TP, None),
    )
    return jax.shard_map(
        shards, mesh=torus, in_specs=placed, out_specs=P(EP, "tp"), check_vma=False
    )
```
